32 devices in a mesh: fs: 4 (over z), rep: 4 (over y, x), tp: 2 (over core).
Axes of the slice: x: 2, y: 2, z: 4, core: 2. Of those that a mesh axis runs over, the one named last changes fastest.
Arguments:
- saved_input: bfloat16 [32768, 2048], P(('fs', 'rep')), may hold values from -8 to 8
- query_cotangent: bfloat16 [32768, 1024], P(('fs', 'rep'), 'tp'), may hold values from -0.03125 to 0.03125
- saved_heads: bfloat16 [32768, 1024], P(('fs', 'rep'), 'tp'), may hold values from -6 to 6
- block_cotangent: bfloat16 [32768, 2048], P(('fs', 'rep')), may hold values from -0.046875 to 0.046875
- query_weight: float32 [2048, 1024], P(('fs', 'rep'), 'tp'), may hold values from -6 to 6
- output_weight: float32 [1024, 2048], P('tp', ('fs', 'rep')), may hold values from -6 to 6
- query_factor: bfloat16 [2048, 256], P(('fs', 'rep')), may hold values from -0.125 to 0.125
- output_factor: bfloat16 [2048, 256], P(('fs', 'rep')), may hold values from -0.125 to 0.125
- query_first: float32 [256, 1024], P(None, 'tp'), may hold values from -6 to 6
- query_second: float32 [256, 1024], P(None, 'tp'), may hold values from 0.5 to 2
- output_first: float32 [1024, 256], P('tp'), may hold values from -6 to 6
- output_second: float32 [1024, 256], P('tp'), may hold values from 0.5 to 2
Outputs:
- new_query_weight: float32 [2048, 1024], P(('fs', 'rep'), 'tp')
- new_output_weight: float32 [1024, 2048], P('tp', ('fs', 'rep'))
- new_query_first: float32 [256, 1024], P(None, 'tp')
- new_query_second: float32 [256, 1024], P(None, 'tp')
- new_output_first: float32 [1024, 256], P('tp')
- new_output_second: float32 [1024, 256], P('tp')
- query_step: float32 [2048, 1024], P(('fs', 'rep'), 'tp')
- output_step: float32 [1024, 2048], P('tp', ('fs', 'rep'))
- query_copy: bfloat16 [2048, 1024], P(None, 'tp')
- output_copy: bfloat16 [1024, 2048], P('tp')
The draws below stay inside these ranges and needn't reach their ends.
All inputs are finite; a program needn't handle non-finite values.
Results may differ from the reference program's by a relative error of at most 0.0013.
Values may be sent and summed in bfloat16 or wider, within the bound.
A program may use at most 128 MiB of HBM per device.

```python
import math
import jax
import jax.numpy as jnp
from jax import lax

D = 2048
RANK = 256
SBW = 1024
TOKENS = 32768


def strengthened(array, own_key, source, target, shards_of, factor):
    owner, partner = [(jnp.arange(array.shape[axis_at]) // (array.shape[axis_at] // shards_of)).reshape([-1 if axis == axis_at else 1 for axis in range(array.ndim)]) for axis_at in (source, target)]
    chosen = jax.random.permutation(own_key, shards_of)[partner]
    strong = (owner == chosen) | (owner == (partner + shards_of // 2) % shards_of)
    return jnp.where(strong, factor * array, array)


def block_levels(rng, shape, pieces, least, top_value):
    def one(position, shards_of):
        heights = jax.random.uniform(jax.random.fold_in(jax.random.fold_in(rng, 6), position), (shards_of,), jnp.float32, least / len(pieces), top_value / len(pieces))
        return jnp.repeat(jnp.exp(heights), shape[position] // shards_of).reshape((-1,) + (1,) * (len(shape) - position - 1))

    level = one(*pieces[0])
    for cut in pieces[1:]:
        level = level * one(*cut)
    return level


def normal_values(rng, extent, deviation, bound, cuts=(), dtype=jnp.bfloat16):
    entries = deviation * jax.random.normal(rng, extent, jnp.float32)
    if cuts:
        entries = entries * block_levels(rng, extent, cuts, -0.22, 0.18)
    return jnp.clip(entries, -bound, bound).astype(dtype)


def noise_with(rng, shape, deviation, bound, split, heavy, kind=jnp.bfloat16):
    drawn = deviation * jax.random.normal(rng, shape, jnp.float32)
    if split:
        drawn = drawn * block_levels(rng, shape, split, -0.22, 0.18)
    return jnp.clip(strengthened(drawn, jax.random.fold_in(rng, 3), *heavy), -bound, bound).astype(kind)


def setup_inputs(seed: int = 0) -> dict:
    arg_keys = jax.random.split(jax.random.key(seed), 13)
    return {
        "saved_input": noise_with(arg_keys[0], (TOKENS, D), 1.0, 8.0, ((0, 16),), (0, 1, 16, 2.0)),
        "query_cotangent": normal_values(arg_keys[1], (TOKENS, SBW), (TOKENS ** -0.5), 0.03125, ((0, 16), (1, 2))),
        "saved_heads": normal_values(arg_keys[2], (TOKENS, SBW), 1.0, 6.0, ((0, 16), (1, 2))),
        "block_cotangent": noise_with(arg_keys[3], (TOKENS, D), (TOKENS ** -0.5), 0.046875, ((0, 16),), (0, 1, 16, 2.0)),
        "query_weight": normal_values(arg_keys[4], (D, SBW), 1.0, 6.0, ((0, 16), (1, 2)), jnp.float32),
        "output_weight": normal_values(arg_keys[5], (SBW, D), 1.0, 6.0, ((0, 2), (1, 16)), jnp.float32),
        "query_factor": normal_values(arg_keys[6], (D, RANK), D ** -0.5, 0.125, ((0, 16),)),
        "output_factor": normal_values(arg_keys[7], (D, RANK), D ** -0.5, 0.125, ((0, 16),)),
        "query_first": normal_values(arg_keys[8], (RANK, SBW), 1.0, 6.0, ((1, 2),), jnp.float32),
        "query_second": jnp.clip(jnp.exp(math.log(2.0) - 1.3862944 * jax.random.uniform(arg_keys[9], (RANK, SBW), jnp.float32) ** block_levels(arg_keys[9], (RANK, SBW), ((1, 2),), -0.2, 0.2)), 0.5, 2.0),
        "output_first": normal_values(arg_keys[10], (SBW, RANK), 1.0, 6.0, ((0, 2),), jnp.float32),
        "output_second": jnp.clip(jnp.exp(math.log(2.0) - 1.3862944 * jax.random.uniform(arg_keys[11], (SBW, RANK), jnp.float32) ** block_levels(arg_keys[11], (SBW, RANK), ((0, 2),), -0.2, 0.2)), 0.5, 2.0),
    }


def reference(saved_input, query_cotangent, saved_heads, block_cotangent, query_weight, output_weight, query_factor, output_factor, query_first, query_second, output_first, output_second):
    contract = (((0,), (0,)), ((), ()))
    high = lax.Precision.HIGHEST
    query_grad = lax.dot_general(saved_input, query_cotangent, contract, preferred_element_type=jnp.float32)
    output_grad = lax.dot_general(saved_heads, block_cotangent, contract, preferred_element_type=jnp.float32)
    factor_q = query_factor.astype(jnp.float32)
    factor_o = output_factor.astype(jnp.float32)
    query_proj = jnp.dot(factor_q.T, query_grad, precision=high)
    output_proj = jnp.dot(output_grad, factor_o, precision=high)
    new_query_first = 0.9 * query_first + 0.1 * query_proj
    new_output_first = 0.9 * output_first + 0.1 * output_proj
    new_query_second = 0.95 * query_second + 0.05 * query_proj * query_proj
    new_output_second = 0.95 * output_second + 0.05 * output_proj * output_proj
    query_dir = new_query_first / (jnp.sqrt(new_query_second) + 1e-08)
    output_dir = new_output_first / (jnp.sqrt(new_output_second) + 1e-08)
    query_raw = jnp.dot(factor_q, query_dir, precision=high)
    output_raw = jnp.dot(output_dir, factor_o.T, precision=high)
    query_step = query_raw / jnp.sqrt(jnp.mean(query_raw * query_raw) + 0.01)
    output_step = output_raw / jnp.sqrt(jnp.mean(output_raw * output_raw) + 0.01)
    new_query_weight = query_weight - 0.1 * query_step
    new_output_weight = output_weight - 0.1 * output_step
    return (new_query_weight, new_output_weight, new_query_first, new_query_second, new_output_first, new_output_second, query_step, output_step, new_query_weight.astype(jnp.bfloat16), new_output_weight.astype(jnp.bfloat16))
```

```python
import functools

import jax
import jax.numpy as jnp
from jax import lax
from jax.experimental import pallas as pl
from jax.experimental.pallas import tpu as pltpu
from jax.sharding import PartitionSpec as P

MESH = pl.DeviceIdType.MESH
BF = jnp.bfloat16
F32 = jnp.float32

REACH = 6.0
SPAN = 120.0
PER_LOG = 1.0 / (2.0 * SPAN * 0.6931471805599453)


def split_parts(wide):
    upper = wide.astype(BF)
    lower = (wide - upper.astype(F32)).astype(BF)
    return (upper, lower)


def encode(weight):
    level = jnp.sqrt(jnp.minimum(jnp.abs(weight), REACH) * (1.0 / REACH))
    size = jnp.exp2(level * (2.0 * SPAN) - SPAN)
    return jnp.where(weight < 0, -size, size).astype(BF)


def decode(code):
    wide = code.astype(F32)
    level = jnp.log(jnp.abs(wide)) * PER_LOG + 0.5
    value = (REACH * level) * level
    return jnp.where(wide < 0, -value, value)


def remote(src, dst, send, recv, where):
    return pltpu.make_async_remote_copy(
        src_ref=src, dst_ref=dst, send_sem=send, recv_sem=recv, device_id=where, device_id_type=MESH
    )


def nth_plane(f, nf, j):
    if j == 0:
        return f, 1
    upper = (2 * f) // nf
    near_end = f + upper * (nf - 1 - 2 * f)
    over = jnp.minimum(1, j // (2 * near_end + 1))
    inner_sign = 1 if j % 2 else -1
    distance = over * (j - near_end) + (1 - over) * ((j + 1) // 2)
    sign = (1 - 2 * upper) * (over + (1 - over) * inner_sign)
    return f + sign * distance, sign


def update_kernel(
    nf, nr, wide, cut,
    x_hbm, bc_hbm, qc_hbm, sh_hbm, wq_hbm, wo_hbm, fq_hbm, fo_hbm, mq_hbm, vq_hbm, mo_hbm, vo_hbm,
    nwq_ref, nwo_ref, nfq_ref, nsq_ref, nfo_ref, nso_ref, stq_ref, sto_ref, cq_ref, co_ref,
    xs, cots, fb, wq_ref, wo_ref, cwq, cwo, low, lows,
    outgoing, landed, own, partial, exchanged, whole, dirs, flat, square,
    loc, fz_s, fz_r, fn_s, fn_r, fd_s, fd_r, fp_s, fp_r, wn_s, wn_r, wd_s, wd_r, wz_s, wz_r,
    a_s, a_r, b_s, b_r, c_s, c_r, e_s, e_r, x_s, x_r,
):
    f, r, t = lax.axis_index("fs"), lax.axis_index("rep"), lax.axis_index("tp")
    near = r + 1 - 2 * lax.rem(r, 2)
    side = lax.rem(r + 2, 4)
    far = 3 - r
    n = nf * nr
    me = f * nr + r
    depth, rank = fq_hbm.shape
    cols = wq_hbm.shape[1]
    tokens = x_hbm.shape[0]
    lane = nr * depth
    quarter = 2 * rank // nr
    rows = quarter // nf
    peers = (near, side, far)
    aligned = depth % 128 == 0

    local = []

    def fetch(src, dst):
        copy = pltpu.make_async_copy(src, dst, loc.at[len(local)])
        copy.start()
        local.append(copy)
        return copy

    small = [fetch(fq_hbm, fb.at[0, me]), fetch(fo_hbm, fb.at[1, me])]
    weights = [fetch(wq_hbm, wq_ref), fetch(wo_hbm, wo_ref)]
    barrier = pltpu.get_barrier_semaphore()
    for df in range(1, nf):
        pl.semaphore_signal(barrier, inc=1, device_id={"fs": lax.rem(f + df, nf)}, device_id_type=MESH)
    for peer in peers:
        pl.semaphore_signal(barrier, inc=1, device_id={"rep": peer}, device_id_type=MESH)
    pl.semaphore_signal(barrier, inc=1, device_id={"tp": 1 - t}, device_id_type=MESH)
    big = [fetch(x_hbm, xs.at[0]), fetch(bc_hbm, xs.at[1]), fetch(qc_hbm, cots.at[0]), fetch(sh_hbm, cots.at[1])]
    moments = [fetch(a, b) for a, b in ((mq_hbm, nfq_ref), (vq_hbm, nsq_ref), (mo_hbm, nfo_ref), (vo_hbm, nso_ref))]
    for copy in small:
        copy.wait()
    pl.semaphore_wait(barrier, nf - 1 + 4)

    sent = []

    def send(src, dst, send_sem, recv_sem, where, when=None):
        def make():
            return remote(src, dst, send_sem, recv_sem, where)

        if when is None:
            make().start()
        else:
            pl.when(when)(lambda: make().start())
        sent.append((make, when))

    def arrive(ref, send_sem, recv_sem):
        remote(ref, ref, send_sem, recv_sem, {"tp": 1 - t}).wait_recv()

    planes = [nth_plane(f, nf, j) for j in range(nf)]

    def fpiece(slot, h):
        return fb.at[t, slot, pl.ds(h * (depth // 2), depth // 2)]

    def f_pass(slot):
        send(fb.at[t, slot], fb.at[t, slot], fp_s.at[slot], fp_r.at[slot], {"tp": 1 - t})

    def f_relay(p):
        slot = p * nr + r
        for h in range(2):
            for k, peer, piece in ((0, near, h), (1, side, 1 - h)):
                ref = fpiece(slot, piece)
                send(ref, ref, fn_s.at[k, p, piece], fn_r.at[k, p, piece], {"rep": peer})

    def f_far(p):
        one, two = p * nr + near, p * nr + side
        for k, slot, piece, to in ((0, one, 0, side), (1, two, 1, near)):
            ref = fpiece(slot, piece)
            arrive(ref, fn_s.at[k, p, piece], fn_r.at[k, p, piece])
            send(ref, ref, fd_s.at[p, piece], fd_r.at[p, piece], {"rep": to})
        for k, slot, piece in ((0, one, 1), (1, two, 0)):
            arrive(fpiece(slot, piece), fn_s.at[k, p, piece], fn_r.at[k, p, piece])
            f_pass(slot)

    def f_done(p):
        slot = p * nr + far
        for piece in range(2):
            arrive(fpiece(slot, piece), fd_s.at[p, piece], fd_r.at[p, piece])
        f_pass(slot)

    def f_tp(p):
        for row in ((near, side, far) if p is f else (r, near, side, far)):
            slot = p * nr + row
            ref = fb.at[1 - t, slot]
            arrive(ref, fp_s.at[slot], fp_r.at[slot])

    def wpiece(slot, p):
        if p == 0:
            return cwq.at[slot, :, pl.ds(0, cut)]
        if p == 2:
            return cwq.at[slot, :, pl.ds(cut, cols - cut)]
        at = pl.ds(0, cut) if p == 1 else pl.ds(cut, cols - cut)
        return cwo.at[slot, at] if aligned else cwo.at[slot, :, at]

    def w_xy(p, pieces):
        for piece in pieces:
            ref = wpiece(p * nr + r, piece)
            for k, peer in ((0, near), (1, side)):
                send(ref, ref, wn_s.at[k, p, piece], wn_r.at[k, p, piece], {"rep": peer})

    def w_far(p, pieces):
        one, two = p * nr + near, p * nr + side
        for piece in pieces:
            k, slot, to = ((0, one, side), (1, two, near))[piece % 2]
            ref = wpiece(slot, piece)
            arrive(ref, wn_s.at[k, p, piece], wn_r.at[k, p, piece])
            send(ref, ref, wd_s.at[p, piece], wd_r.at[p, piece], {"rep": to})

    def w_rest(p, pieces):
        one, two = p * nr + near, p * nr + side
        for piece in pieces:
            k, slot = ((1, two), (0, one))[piece % 2]
            ref = wpiece(slot, piece)
            arrive(ref, wn_s.at[k, p, piece], wn_r.at[k, p, piece])

    def w_last(p, pieces):
        for piece in pieces:
            ref = wpiece(p * nr + far, piece)
            arrive(ref, wd_s.at[p, piece], wd_r.at[p, piece])

    items = {0: ((0, 0), (1, 1), (2, 2), (3, 3)), 1: ((4, 0), (5, 1)), 2: ((6, 0), (7, 1)), 3: ((8, 0), (9, 1))}
    row_of = (r, near, side, far)

    def w_zown(*roles):
        for role in roles:
            for item, piece in items[role]:
                ref = wpiece(f * nr + row_of[role], piece)
                send(ref, ref, wz_s.at[f, item], wz_r.at[f, item], {"fs": f + 1}, f < nf - 1)
                send(ref, ref, wz_s.at[nf, item], wz_r.at[f, item], {"fs": f - 1}, f > 0)

    def w_zpass(j, *roles):
        p, sign = planes[j]
        to = f - sign
        for role in roles:
            for item, piece in items[role]:
                ref = wpiece(p * nr + row_of[role], piece)
                arrive(ref, wz_s.at[p, item], wz_r.at[p, item])
                inside = jnp.logical_and(to >= 0, to < nf)
                send(ref, ref, wz_s.at[p, item], wz_r.at[p, item], {"fs": to}, inside)

    def lowered(j):
        p = planes[j][0]
        for which in range(2):
            block = fb[which, pl.ds(p * nr, nr)].reshape(lane, rank)
            step = tokens // 2

            def one(i, carry):
                at = pl.ds(pl.multiple_of(i * step, 256), step)
                got = jnp.dot(
                    xs[which, at, pl.ds(pl.multiple_of(p * lane, 128), lane)], block, preferred_element_type=F32
                )
                if j > 0:
                    got = got + low[which, at]
                if j == nf - 1:
                    upper, lower = split_parts(got)
                    lows[0, at, which * rank : (which + 1) * rank] = upper
                    lows[1, at, which * rank : (which + 1) * rank] = lower
                else:
                    low[which, at] = got
                return carry

            lax.fori_loop(0, 2, one, 0)

    for df in range(1, nf):
        to = planes[df][0]
        ref = fb.at[t, me]
        send(ref, ref, fz_s.at[to], fz_r.at[f], {"fs": to})
    f_relay(f)
    for copy in weights:
        copy.wait()
    cwq[me] = encode(wq_ref[...])
    cwo[me] = encode(wo_ref[...]) if aligned else encode(wo_ref[...].T)
    w_xy(f, (0, 1))
    for j in range(1, nf):
        p = planes[j][0]
        slot = p * nr + r
        arrive(fb.at[t, slot], fz_s.at[p], fz_r.at[p])
        f_relay(p)
        f_pass(slot)
        if j == 1:
            w_zown(0)
        f_far(planes[j - 1][0])
        if j == 2:
            w_far(f, (0, 1))
            w_rest(f, (0, 1))
            w_zown(1, 2)
            for copy in big:
                copy.wait()
        if j == 3:
            w_last(f, (0, 1))
            w_zown(3)
        if j >= 2:
            f_done(planes[j - 2][0])
            f_tp(planes[j - 2][0])
            lowered(j - 2)
    f_far(planes[nf - 1][0])
    w_xy(f, (2, 3))
    f_done(planes[nf - 2][0])
    f_tp(planes[nf - 2][0])
    lowered(nf - 2)
    w_zpass(1, 0)
    f_done(planes[nf - 1][0])
    f_tp(planes[nf - 1][0])
    lowered(nf - 1)

    contract = (((0,), (0,)), ((), ()))
    for k, peer in ((2, far), (0, near), (1, side), (None, r)):
        at = pl.ds(pl.multiple_of(peer * quarter, 128), quarter)
        cot = cots[(peer * quarter) // rank]
        part = lax.dot_general(lows[0, :, at], cot, contract, preferred_element_type=F32) + lax.dot_general(
            lows[1, :, at], cot, contract, preferred_element_type=F32
        )
        part = part.reshape(nf, rows, cols)
        if k is None:
            own[...] = part
        else:
            outgoing[k] = part.astype(BF)
            send(outgoing.at[k], landed.at[k], a_s.at[k], a_r.at[k], {"rep": peer})
    w_far(f, (2, 3))
    w_xy(planes[1][0], (2, 3))
    w_zpass(1, 1, 2, 3)
    for k in range(3):
        arrive(landed.at[k], a_s.at[k], a_r.at[k])
    total = own[...] + landed[0].astype(F32) + landed[1].astype(F32) + landed[2].astype(F32)
    partial[...] = total.astype(BF)
    own[...] = total
    for j in range(1, nf):
        to = planes[j][0]
        send(partial.at[to], exchanged.at[f], b_s.at[to], b_r.at[f], {"fs": to})
    w_far(planes[1][0], (2, 3))
    mine = own[f]
    for j in range(1, nf):
        p = planes[j][0]
        arrive(exchanged.at[p], b_s.at[p], b_r.at[p])
        mine = mine + exchanged[p].astype(F32)
    whole[r, f] = mine.astype(BF)
    for j in range(nf):
        p = planes[j][0]
        ref = whole.at[r, p]
        if j == 0:
            for i in range(1, nf):
                to = planes[i][0]
                send(ref, ref, c_s.at[to], c_r.at[f], {"fs": to})
        else:
            arrive(ref, c_s.at[p], c_r.at[p])
        for k, peer in ((2, far), (0, near), (1, side)):
            send(ref, ref, e_s.at[k, p], e_r.at[k, p], {"rep": peer})
    w_zpass(2, 0)
    w_xy(planes[2][0], (2, 3))
    w_zpass(2, 1, 2, 3)
    for j in range(nf):
        p = planes[j][0]
        for k, peer in enumerate(peers):
            arrive(whole.at[peer, p], e_s.at[k, p], e_r.at[k, p])
    for copy in moments:
        copy.wait()
    half = nr // 2
    for which, first_ref, second_ref in ((0, nfq_ref, nsq_ref), (1, nfo_ref, nso_ref)):
        proj = whole[which * half : (which + 1) * half].astype(F32).reshape(rank, cols)
        if which:
            proj = proj.T
        moved = 0.9 * first_ref[...] + 0.1 * proj
        spread = 0.95 * second_ref[...] + 0.05 * proj * proj
        first_ref[...] = moved
        second_ref[...] = spread
        way = moved / (jnp.sqrt(spread) + 1e-08)
        upper, lower = split_parts(way)
        if which:
            flat[:, 0:rank] = upper
            flat[:, rank : 2 * rank] = lower
        else:
            dirs[0:rank] = upper
            dirs[rank : 2 * rank] = lower

    for j in range(3, nf):
        w_zpass(j, 0)
        w_xy(planes[j][0], (2, 3))
        w_far(planes[j - 1][0], (2, 3))

    def doubled(which, at, count):
        block = fb[which, pl.ds(at, count)].reshape(count * depth, rank)
        return jnp.concatenate([block, block], axis=1)

    across = (((1,), (1,)), ((), ()))

    def raw_q(at, count):
        return jnp.dot(doubled(0, at, count), dirs[...], preferred_element_type=F32)

    def raw_o(at, count):
        return lax.dot_general(flat[...], doubled(1, at, count), across, preferred_element_type=F32)

    def add(i, carry):
        one, two = carry
        raw = raw_q(i * nr, nr)
        one = one + jnp.sum((raw * raw).reshape(lane // 8, 8, cols), axis=0)
        raw = raw_o(i * nr, nr)
        two = two + jnp.sum((raw * raw).reshape(cols // 8, 8, lane), axis=0)
        return one, two

    one, two = lax.fori_loop(0, nf, add, (jnp.zeros((8, cols), F32), jnp.zeros((8, lane), F32)))
    square[0, 0] = jnp.full((8, 128), jnp.sum(one), F32)
    square[0, 1] = jnp.full((8, 128), jnp.sum(two), F32)
    copy = remote(square.at[0], square.at[1], x_s, x_r, {"tp": 1 - t})
    copy.start()
    for j in range(3, nf):
        w_zpass(j, 1, 2, 3)
    w_far(planes[nf - 1][0], (2, 3))
    copy.wait()
    entries = wide * cols * 2
    scale = [
        1.0 / jnp.sqrt((square[0, which, 0:1, 0:1] + square[1, which, 0:1, 0:1]) / entries + 0.01) for which in range(2)
    ]
    for raw, weight, new_weight, step_ref, which in (
        (raw_q(me, 1), wq_ref, nwq_ref, stq_ref, 0),
        (raw_o(me, 1), wo_ref, nwo_ref, sto_ref, 1),
    ):
        step = raw * scale[which]
        step_ref[...] = step
        new_weight[...] = weight[...] - 0.1 * step

    rate = [0.1 * scale[which] for which in range(2)]

    def finish(p):
        at = p * nr
        raw = raw_q(at, nr).reshape(nr, depth, cols)
        cq_ref[pl.ds(at, nr)] = (decode(cwq[pl.ds(at, nr)]) - rate[0] * raw).astype(BF)
        raw = raw_o(at, nr)
        if aligned:
            for k in range(nr):
                new = decode(cwo[at + k]) - rate[1] * raw[:, k * depth : (k + 1) * depth]
                co_ref[:, pl.ds(pl.multiple_of((at + k) * depth, 128), depth)] = new.astype(BF)
        else:
            new = decode(cwo[pl.ds(at, nr)]).reshape(lane, cols).T - rate[1] * raw
            co_ref[:, pl.ds(pl.multiple_of(p * lane, 128), lane)] = new.astype(BF)

    for j in range(nf):
        p = planes[j][0]
        w_rest(p, (2, 3))
        w_last(p, (2, 3))
        finish(p)
    for make, when in sent:
        if when is None:
            make().wait_send()
        else:
            pl.when(when)(lambda make=make: make().wait_send())


def store_kernel(count, *refs):
    ins, outs, sems = refs[:count], refs[count : 2 * count], refs[2 * count]
    copies = [pltpu.make_async_copy(ins[k], outs[k], sems.at[k]) for k in range(count)]
    for copy in copies:
        copy.start()
    for copy in copies:
        copy.wait()


def store(arrays):
    count = len(arrays)
    return pl.pallas_call(
        functools.partial(store_kernel, count),
        out_shape=[jax.ShapeDtypeStruct(a.shape, a.dtype) for a in arrays],
        in_specs=[pl.BlockSpec(memory_space=pltpu.VMEM)] * count,
        out_specs=[pl.BlockSpec(memory_space=pl.ANY)] * count,
        scratch_shapes=[pltpu.SemaphoreType.DMA((count,))],
        compiler_params=pltpu.CompilerParams(vmem_limit_bytes=16 * 1024 * 1024),
    )(*arrays)


def body(nf, nr, *args):
    saved_input, query_cotangent, saved_heads, block_cotangent, query_weight, output_weight = args[:6]
    query_factor, output_factor, query_first, query_second, output_first, output_second = args[6:]
    n = nf * nr
    depth, rank = query_factor.shape
    cols = query_weight.shape[1]
    tokens, width = saved_input.shape
    quarter = 2 * rank // nr
    rows = quarter // nf
    cut = cols // 4
    aligned = depth % 128 == 0
    dma = pltpu.SemaphoreType.DMA
    vmem = pl.BlockSpec(memory_space=pltpu.VMEM)
    shape = jax.ShapeDtypeStruct
    args = [pltpu.with_memory_space_constraint(a, pltpu.HBM) for a in args]
    outs = pl.pallas_call(
        functools.partial(update_kernel, nf, nr, n * depth, cut),
        out_shape=[
            shape((depth, cols), F32), shape((cols, depth), F32),
            shape((rank, cols), F32), shape((rank, cols), F32),
            shape((cols, rank), F32), shape((cols, rank), F32),
            shape((depth, cols), F32), shape((cols, depth), F32),
            shape((n, depth, cols), BF),
            shape((cols, n * depth), BF),
        ],
        in_specs=[pl.BlockSpec(memory_space=pltpu.HBM)] * 12,
        out_specs=[vmem] * 10,
        scratch_shapes=[
            pltpu.VMEM((2, tokens, width), BF),
            pltpu.VMEM((2, tokens, cols), BF),
            pltpu.VMEM((2, n, depth, rank), BF),
            pltpu.VMEM((depth, cols), F32), pltpu.VMEM((cols, depth), F32),
            pltpu.VMEM((n, depth, cols), BF), pltpu.VMEM((n, cols, depth) if aligned else (n, depth, cols), BF),
            pltpu.VMEM((2, tokens, rank), F32),
            pltpu.VMEM((2, tokens, 2 * rank), BF),
            pltpu.VMEM((3, nf, rows, cols), BF), pltpu.VMEM((3, nf, rows, cols), BF),
            pltpu.VMEM((nf, rows, cols), F32), pltpu.VMEM((nf, rows, cols), BF),
            pltpu.VMEM((nf, rows, cols), BF), pltpu.VMEM((nr, nf, rows, cols), BF),
            pltpu.VMEM((2 * rank, cols), BF), pltpu.VMEM((cols, 2 * rank), BF),
            pltpu.VMEM((2, 2, 8, 128), F32),
            dma((12,)),
            dma((nf,)), dma((nf,)), dma((2, nf, 2)), dma((2, nf, 2)), dma((nf, 2)), dma((nf, 2)), dma((n,)), dma((n,)),
            dma((2, nf, 4)), dma((2, nf, 4)), dma((nf, 4)), dma((nf, 4)), dma((nf + 1, 10)), dma((nf, 10)),
            dma((3,)), dma((3,)), dma((nf,)), dma((nf,)), dma((nf,)), dma((nf,)), dma((3, nf)), dma((3, nf)), dma, dma,
        ],
        compiler_params=pltpu.CompilerParams(
            collective_id=0, has_side_effects=True, vmem_limit_bytes=(44 if aligned else 52) * 1024 * 1024
        ),
    )(*[args[k] for k in (0, 3, 1, 2, 4, 5, 6, 7, 8, 9, 10, 11)])
    *rest, query_copy, output_copy = store(outs)
    return (*rest, query_copy.reshape(n * depth, cols), output_copy)


def solution(mesh):
    nf, nr = mesh.shape["fs"], mesh.shape["rep"]
    in_specs = (
        P(("fs", "rep"), None), P(("fs", "rep"), "tp"), P(("fs", "rep"), "tp"), P(("fs", "rep"), None),
        P(("fs", "rep"), "tp"), P("tp", ("fs", "rep")), P(("fs", "rep"), None), P(("fs", "rep"), None),
        P(None, "tp"), P(None, "tp"), P("tp", None), P("tp", None),
    )
    out_specs = (
        P(("fs", "rep"), "tp"), P("tp", ("fs", "rep")), P(None, "tp"), P(None, "tp"), P("tp", None), P("tp", None),
        P(("fs", "rep"), "tp"), P("tp", ("fs", "rep")), P(None, "tp"), P("tp", None),
    )
    return jax.shard_map(
        functools.partial(body, nf, nr), mesh=mesh, in_specs=in_specs, out_specs=out_specs, check_vma=False
    )
```

```python
import functools

import jax
import jax.numpy as jnp
from jax import lax
from jax.experimental import pallas as pl
from jax.experimental.pallas import tpu as pltpu
from jax.sharding import PartitionSpec as P

MESH = pl.DeviceIdType.MESH
BF = jnp.bfloat16
F32 = jnp.float32

REACH = 6.0
SPAN = 120.0
PER_LOG = 1.0 / (2.0 * SPAN * 0.6931471805599453)


def split_parts(wide):
    upper = wide.astype(BF)
    lower = (wide - upper.astype(F32)).astype(BF)
    return (upper, lower)


def encode(weight):
    level = jnp.sqrt(jnp.minimum(jnp.abs(weight), REACH) * (1.0 / REACH))
    size = jnp.exp2(level * (2.0 * SPAN) - SPAN)
    return jnp.where(weight < 0, -size, size).astype(BF)


def decode(code):
    wide = code.astype(F32)
    level = jnp.log(jnp.abs(wide)) * PER_LOG + 0.5
    value = (REACH * level) * level
    return jnp.where(wide < 0, -value, value)


def remote(src, dst, send, recv, where):
    return pltpu.make_async_remote_copy(
        src_ref=src, dst_ref=dst, send_sem=send, recv_sem=recv, device_id=where, device_id_type=MESH
    )


def nth_plane(f, nf, j):
    if j == 0:
        return f, 0
    upper = (2 * f) // nf
    near_end = f + upper * (nf - 1 - 2 * f)
    over = jnp.minimum(1, j // (2 * near_end + 1))
    inner_sign = 1 if j % 2 else -1
    distance = over * (j - near_end) + (1 - over) * ((j + 1) // 2)
    sign = (1 - 2 * upper) * (over + (1 - over) * inner_sign)
    return f + sign * distance, distance


def update_kernel(
    nf, nr, wide,
    x_hbm, bc_hbm, qc_hbm, sh_hbm, wq_hbm, wo_hbm, fq_hbm, fo_hbm, mq_hbm, vq_hbm, mo_hbm, vo_hbm,
    nwq_out, nwo_out, nfq_out, nsq_out, nfo_out, nso_out, stq_out, sto_out, cq_out, co_out,
    nwq_ref, nwo_ref, nfq_ref, nsq_ref, nfo_ref, nso_ref, stq_ref, sto_ref, cq_ref, co_ref,
    xs, cots, fb, wq_ref, wo_ref, cwq, cwo, low, lows,
    mine, outgoing, landed, partial, exchanged, whole, dirs, flat, gram_q, gram_o, square,
    loc, put_s, fz_s, fz_r, fn_s, fn_r, fd_s, fd_r, fp_s, fp_r, wn_s, wn_r, wd_s, wd_r, wz_s, wz_r, wb_s, wb_r,
    a_s, a_r, b_s, b_r, c_s, c_r, e_s, e_r, g_s, g_r, h_s, h_r, x_s, x_r,
):
    f, r, t = lax.axis_index("fs"), lax.axis_index("rep"), lax.axis_index("tp")
    near = r + 1 - 2 * lax.rem(r, 2)
    side = lax.rem(r + 2, 4)
    far = 3 - r
    n = nf * nr
    me = f * nr + r
    depth, rank = fq_hbm.shape
    cols = wq_hbm.shape[1]
    tokens = x_hbm.shape[0]
    lane = nr * depth
    rows = rank // nf
    half = nr // 2
    span = cols // half
    peers = (near, side, far)
    aligned = depth % 128 == 0

    local = []

    def fetch(src, dst):
        copy = pltpu.make_async_copy(src, dst, loc.at[len(local)])
        copy.start()
        local.append(copy)
        return copy

    small = [fetch(fq_hbm, fb.at[0, me]), fetch(fo_hbm, fb.at[1, me])]
    weights = [fetch(wq_hbm, wq_ref), fetch(wo_hbm, wo_ref)]
    barrier = pltpu.get_barrier_semaphore()
    for df in range(1, nf):
        pl.semaphore_signal(barrier, inc=1, device_id={"fs": lax.rem(f + df, nf)}, device_id_type=MESH)
    for peer in peers:
        pl.semaphore_signal(barrier, inc=1, device_id={"rep": peer}, device_id_type=MESH)
    pl.semaphore_signal(barrier, inc=1, device_id={"tp": 1 - t}, device_id_type=MESH)
    first, second = t == 0, t == 1
    base = len(local)
    big = []
    for k, (when, src, dst) in enumerate((
        (first, x_hbm, xs), (second, bc_hbm, xs), (first, qc_hbm, cots.at[t]), (second, sh_hbm, cots.at[t]),
    )):
        def make(src=src, dst=dst, k=k):
            return pltpu.make_async_copy(src, dst, loc.at[base + k // 2])

        pl.when(when)(lambda make=make: make().start())
        big.append((when, make))
    local.extend(big[:2])
    moments = [fetch(a, b) for a, b in ((mq_hbm, nfq_ref), (vq_hbm, nsq_ref), (mo_hbm, nfo_ref), (vo_hbm, nso_ref))]
    for copy in small:
        copy.wait()
    pl.semaphore_wait(barrier, nf - 1 + 4)

    def put(src, dst, kind):
        pltpu.make_async_copy(src, dst, put_s.at[kind]).start()

    def gated(when, act):
        if when is None:
            act()
        else:
            pl.when(when)(act)

    def send(src, dst, send_sem, recv_sem, where, when=None):
        gated(when, lambda: remote(src, dst, send_sem, recv_sem, where).start())

    def arrive(ref, sem):
        remote(ref, ref, sem, sem, {"tp": 1 - t}).wait_recv()

    def settle(ref, sem, when=None):
        gated(when, lambda: remote(ref, ref, sem, sem, {"tp": 1 - t}).wait_send())

    def blocks(count):
        return cwq.at[pl.ds(0, count)]

    planes = [nth_plane(f, nf, j) for j in range(nf)]
    for when, src in ((first, sh_hbm), (second, qc_hbm)):
        send(src, cots.at[t], h_s, h_r, {"tp": 1 - t}, when)

    def fpiece(slot, h):
        return fb.at[t, slot, pl.ds(h * (depth // 2), depth // 2)]

    def f_pass(slot):
        send(fb.at[t, slot], fb.at[t, slot], fp_s, fp_r, {"tp": 1 - t})

    def f_relay(p):
        slot = p * nr + r
        for h in range(2):
            for k, peer, piece in ((0, near, h), (1, side, 1 - h)):
                ref = fpiece(slot, piece)
                send(ref, ref, fn_s, fn_r.at[k if piece == k else 2, p], {"rep": peer})

    def f_far(p):
        one, two = p * nr + near, p * nr + side
        for piece, slot, to in ((0, one, side), (1, two, near)):
            ref = fpiece(slot, piece)
            arrive(ref, fn_r.at[piece, p])
            send(ref, ref, fd_s, fd_r.at[p], {"rep": to})
        arrive(fb.at[t, one], fn_r.at[2, p])
        f_pass(one)
        f_pass(two)

    def f_done(p):
        slot = p * nr + far
        arrive(fb.at[t, slot], fd_r.at[p])
        f_pass(slot)

    def wpiece(slot, p):
        ref, count = ((cwq, depth), (cwo, cols if aligned else depth))[p % 2]
        return ref.at[slot, pl.ds(p // 2 * (count // 2), count // 2)]

    def chosen(j, pieces):
        for piece in pieces:
            if piece >= 2 or j == 0:
                yield piece, None
            elif j > 1:
                yield piece, planes[j][1] > 1

    def w_xy(j, pieces):
        p = planes[j][0]
        for piece, when in chosen(j, pieces):
            ref = wpiece(p * nr + r, piece)
            for k, peer in ((0, near), (1, side)):
                at = piece // 2 if piece % 2 == k else 2
                send(ref, ref, wn_s.at[p], wn_r.at[k, p, at], {"rep": peer}, when)

    def w_far(j, pieces):
        p = planes[j][0]
        one, two = p * nr + near, p * nr + side
        for piece, when in chosen(j, pieces):
            k = piece % 2
            ref = wpiece((one, two)[k], piece)
            gated(when, lambda: arrive(ref, wn_r.at[k, p, piece // 2]))
            send(ref, ref, wd_s.at[p], wd_r.at[p, piece // 2], {"rep": (side, near)[k]}, when)

    def w_rest(j):
        p, distance = planes[j]
        for k, ref in ((0, cwo.at[p * nr + near]), (1, cwq.at[p * nr + side])):
            part = wpiece(p * nr + (near, side)[k], 3 - k)
            if j != 1:
                gated(None if j == 0 else distance > 1, lambda: arrive(ref, wn_r.at[k, p, 2]))
            if j > 0:
                gated(distance == 1, lambda: arrive(part, wn_r.at[k, p, 2]))

    def w_last(j, half_of):
        p, distance = planes[j]
        if half_of or j != 1:
            when = None if half_of or j == 0 else distance > 1
            gated(when, lambda: arrive(cwq.at[p * nr + far], wd_r.at[p, half_of]))

    def w_out(j, when=None):
        to = planes[j][0]
        for piece in (2, 3, 0, 1):
            ref = wpiece(me, piece)
            send(ref, ref, wz_s, wz_r.at[f], {"fs": to}, when)

    def w_in(j):
        arrive(blocks(2), wz_r.at[planes[j][0]])

    def w_beside():
        for row in (near, side, far):
            for piece in (0, 1):
                ref = wpiece(f * nr + row, piece)
                send(ref, ref, wb_s.at[0], wb_r.at[f], {"fs": f + 1}, f < nf - 1)
                send(ref, ref, wb_s.at[1], wb_r.at[f], {"fs": f - 1}, f > 0)

    def lowered(j):
        p = planes[j][0]
        block = fb[t, pl.ds(p * nr, nr)].reshape(lane, rank)
        return jnp.dot(xs[:, pl.ds(pl.multiple_of(p * lane, 128), lane)], block, preferred_element_type=F32)

    for j in range(1, nf):
        to = planes[j][0]
        ref = fb.at[t, me]
        send(ref, ref, fz_s, fz_r.at[f], {"fs": to})
    f_relay(f)
    for copy in weights:
        copy.wait()
    cwq[me] = encode(wq_ref[...])
    cwo[me] = encode(wo_ref[...]) if aligned else encode(wo_ref[...].T)
    w_xy(0, (0,))
    for j in range(1, nf):
        p = planes[j][0]
        slot = p * nr + r
        arrive(fb.at[t, slot], fz_r.at[p])
        f_relay(p)
        f_pass(slot)
        if j == 1:
            w_xy(0, (1,))
        if j == nf - 1:
            for k in range(1, nf):
                w_out(k, planes[k][1] <= 2 if k > 2 else None)
        f_far(planes[j - 1][0])
    for j in range(nf - 2):
        f_done(planes[j][0])
    f_far(planes[nf - 1][0])
    w_xy(0, (2, 3))
    w_far(0, (0, 1))
    f_done(planes[nf - 2][0])
    for when, make in big:
        pl.when(when)(lambda make=make: make().wait())
    low[...] = sum(lowered(j) for j in range(nf - 1))
    f_done(planes[nf - 1][0])
    w_far(0, (2,))
    w_in(1)
    w_xy(1, (2, 3))
    lows[...] = (low[...] + lowered(nf - 1)).astype(BF)
    w_far(0, (3,))
    arrive(cots.at[1 - t], h_r)
    contract = (((0,), (0,)), ((), ()))
    for side_of, quarters in ((side // half, ((2, far), (1, side))), (r // half, ((0, near),))):
        part = lax.dot_general(lows[...], cots[side_of], contract, preferred_element_type=F32)
        for k in range(half):
            block = part[:, k * span : (k + 1) * span].reshape(nf, rows, span)
            mine[side_of * half + k] = block
            outgoing[side_of * half + k] = block.astype(BF)
        for k, peer in quarters:
            for j in range(nf - 1, -1, -1):
                p = planes[j][0]
                send(outgoing.at[peer, p], landed.at[k, p], a_s, a_r.at[p], {"rep": peer})
    w_last(0, 0)
    for j in range(nf - 1, -1, -1):
        p = planes[j][0]
        arrive(landed.at[:, p], a_r.at[p])
        total = mine[r, p] + landed[0, p].astype(F32) + landed[1, p].astype(F32) + landed[2, p].astype(F32)
        if j > 0:
            partial[p] = total.astype(BF)
            send(partial.at[p], exchanged.at[f], b_s, b_r.at[f], {"fs": p})
        else:
            result = total
    def hand(row):
        ref = whole.at[t, row]
        send(ref, ref, g_s, g_r, {"tp": 1 - t}, row // half == 1 - t)

    w_far(1, (2, 3))
    w_in(2)
    w_xy(2, (2, 3))
    for j in range(1, nf):
        p = planes[j][0]
        arrive(exchanged.at[p], b_r.at[p])
        result = result + exchanged[p].astype(F32)
    whole[t, r, f] = result.astype(BF)
    for j in range(nf):
        p = planes[j][0]
        ref = whole.at[t, r, p]
        if j == 0:
            for i in range(1, nf):
                to = planes[i][0]
                send(ref, ref, c_s, c_r.at[f], {"fs": to})
        else:
            arrive(ref, c_r.at[p])
        for k, peer in ((2, far), (0, near), (1, side)):
            send(ref, ref, e_s, e_r.at[k], {"rep": peer})
        if j == 0:
            for i in range(3, nf):
                w_out(i, planes[i][1] > 2)
    hand(r)
    w_far(2, (2, 3))
    w_xy(2, (0, 1))
    w_rest(0)
    w_beside()
    arrive(fb.at[1 - t, pl.ds(0, n - 1)], fp_r)
    for which in range(2):
        block = fb[which].reshape(wide, rank)
        upper, lower = split_parts(lax.dot_general(block, block, contract, preferred_element_type=F32))
        if which:
            gram_o[...] = jnp.concatenate([upper, lower, upper], axis=0)
        else:
            gram_q[...] = jnp.concatenate([upper, lower, upper], axis=1)
    for j in range(3, nf):
        w_in(j)
        w_xy(j, (2, 3))
    for k, peer in ((0, near), (1, side), (2, far)):
        arrive(whole.at[t, peer], e_r.at[k])
        hand(peer)
    arrive(whole.at[1 - t, pl.ds(t * half, half)], g_r)
    for copy in moments:
        copy.wait()
    norms = []
    for which, first_ref, second_ref in ((0, nfq_ref, nsq_ref), (1, nfo_ref, nso_ref)):
        proj = jnp.concatenate(
            [whole[which, t * half + k].astype(F32).reshape(rank, span) for k in range(half)], axis=1
        )
        if which:
            proj = proj.T
        moved = 0.9 * first_ref[...] + 0.1 * proj
        spread = 0.95 * second_ref[...] + 0.05 * proj * proj
        first_ref[...] = moved
        second_ref[...] = spread
        way = moved / (jnp.sqrt(spread) + 1e-08)
        upper, lower = split_parts(way)
        if which:
            flat[:, 0:rank] = upper
            flat[:, rank : 2 * rank] = lower
            shaped = jnp.dot(
                jnp.concatenate([upper, upper, lower], axis=1), gram_o[...], preferred_element_type=F32
            )
        else:
            dirs[0:rank] = upper
            dirs[rank : 2 * rank] = lower
            shaped = jnp.dot(
                gram_q[...], jnp.concatenate([upper, upper, lower], axis=0), preferred_element_type=F32
            )
        norms.append(jnp.sum(shaped * way))

    for src, dst in ((nfq_ref, nfq_out), (nsq_ref, nsq_out), (nfo_ref, nfo_out), (nso_ref, nso_out)):
        put(src, dst, 0)
    w_far(2, (0, 1))
    for j in range(3, nf):
        w_xy(j, (0, 1))

    def doubled(which, at, count):
        block = fb[which, pl.ds(at, count)].reshape(count * depth, rank)
        return jnp.concatenate([block, block], axis=1)

    across = (((1,), (1,)), ((), ()))

    def raw_q(at, count):
        return jnp.dot(doubled(0, at, count), dirs[...], preferred_element_type=F32)

    def raw_o(at, count):
        return lax.dot_general(flat[...], doubled(1, at, count), across, preferred_element_type=F32)

    square[0, 0] = jnp.full((8, 128), norms[0], F32)
    square[0, 1] = jnp.full((8, 128), norms[1], F32)
    copy = remote(square.at[0], square.at[1], x_s, x_r, {"tp": 1 - t})
    copy.start()
    for j in range(3, nf):
        w_far(j, (2, 3))
    copy.wait()
    entries = wide * cols * 2
    scale = [
        1.0 / jnp.sqrt(jnp.maximum(square[0, which, 0:1, 0:1] + square[1, which, 0:1, 0:1], 0.0) / entries + 0.01) for which in range(2)
    ]
    for raw, weight, new_weight, step_ref, which in (
        (raw_q(me, 1), wq_ref, nwq_ref, stq_ref, 0),
        (raw_o(me, 1), wo_ref, nwo_ref, sto_ref, 1),
    ):
        step = raw * scale[which]
        step_ref[...] = step
        new_weight[...] = weight[...] - 0.1 * step

    for src, dst in ((nwq_ref, nwq_out), (nwo_ref, nwo_out), (stq_ref, stq_out), (sto_ref, sto_out)):
        put(src, dst, 1)
    rate = [0.1 * scale[which] for which in range(2)]

    def finish(at, count):
        raw = raw_q(at, count).reshape(count, depth, cols)
        cq_ref[pl.ds(at, count)] = (decode(cwq[pl.ds(at, count)]) - rate[0] * raw).astype(BF)
        raw = raw_o(at, count)
        if aligned:
            for k in range(count):
                new = decode(cwo[at + k]) - rate[1] * raw[:, k * depth : (k + 1) * depth]
                co_ref[:, pl.ds(pl.multiple_of((at + k) * depth, 128), depth)] = new.astype(BF)
        else:
            new = decode(cwo[pl.ds(at, count)]).reshape(count * depth, cols).T - rate[1] * raw
            co_ref[:, pl.ds(pl.multiple_of(at * depth, 128), count * depth)] = new.astype(BF)
        block = pl.ds(at, count)
        put(cq_ref.at[block], cq_out.at[block], 2)
        block = pl.ds(pl.multiple_of(at * depth, 128), count * depth)
        put(co_ref.at[:, block], co_out.at[:, block], 3)

    for j in range(nf - 1):
        p = planes[j][0]
        if j > 0:
            w_rest(j)
            w_last(j, 0)
        w_last(j, 1)
        if j == 1:
            for step, when in ((1, f < nf - 1), (-1, f > 0)):
                gated(when, lambda: arrive(blocks(3), wb_r.at[f + step]))
        finish(p * nr, nr)
    for j in range(3, nf):
        w_far(j, (0, 1))
    p = planes[nf - 1][0]
    w_rest(nf - 1)
    if aligned:
        for row in (r, near, side):
            finish(p * nr + row, 1)
    w_last(nf - 1, 0)
    w_last(nf - 1, 1)
    if aligned:
        finish(p * nr + far, 1)
    else:
        finish(p * nr, nr)
    for kind, ref in ((0, cq_ref), (1, blocks(8)), (2, cq_ref), (3, co_ref)):
        pltpu.make_async_copy(ref, ref, put_s.at[kind]).wait()
    settle(fb.at[t, pl.ds(0, nf - 1)], fz_s)
    settle(fb.at[t, pl.ds(0, 2 * nf)], fn_s)
    settle(fb.at[t, pl.ds(0, nf)], fd_s)
    settle(fb.at[t, pl.ds(0, n - 1)], fp_s)
    for j in range(nf):
        p, distance = planes[j]
        if j != 1:
            full = None if j == 0 else distance > 1
            settle(blocks(4), wn_s.at[p], full)
            settle(blocks(2), wd_s.at[p], full)
        if j > 0:
            settle(blocks(2), wn_s.at[p], distance == 1)
            settle(blocks(1), wd_s.at[p], distance == 1)
    settle(blocks(2 * (nf - 1)), wz_s)
    settle(blocks(3), wb_s.at[0], f < nf - 1)
    settle(blocks(3), wb_s.at[1], f > 0)
    settle(outgoing.at[pl.ds(0, 3)], a_s)
    settle(partial.at[pl.ds(0, nf - 1)], b_s)
    settle(whole.at[t, r, pl.ds(0, nf - 1)], c_s)
    settle(whole.at[t, pl.ds(0, 3)], e_s)
    settle(whole.at[t, pl.ds(0, half)], g_s)
    settle(cots.at[t], h_s)


def store_kernel(count, *refs):
    ins, outs, sems = refs[:count], refs[count : 2 * count], refs[2 * count]
    copies = [pltpu.make_async_copy(ins[k], outs[k], sems.at[k]) for k in range(count)]
    for copy in copies:
        copy.start()
    for copy in copies:
        copy.wait()


def store(arrays):
    count = len(arrays)
    return pl.pallas_call(
        functools.partial(store_kernel, count),
        out_shape=[jax.ShapeDtypeStruct(a.shape, a.dtype) for a in arrays],
        in_specs=[pl.BlockSpec(memory_space=pl.ANY)] * count,
        out_specs=[pl.BlockSpec(memory_space=pl.ANY)] * count,
        scratch_shapes=[pltpu.SemaphoreType.DMA((count,))],
        compiler_params=pltpu.CompilerParams(vmem_limit_bytes=16 * 1024 * 1024),
    )(*arrays)


def body(nf, nr, *args):
    saved_input, query_cotangent, saved_heads, block_cotangent, query_weight, output_weight = args[:6]
    query_factor, output_factor, query_first, query_second, output_first, output_second = args[6:]
    n = nf * nr
    depth, rank = query_factor.shape
    cols = query_weight.shape[1]
    tokens, width = saved_input.shape
    rows = rank // nf
    span = 2 * cols // nr
    aligned = depth % 128 == 0
    dma = pltpu.SemaphoreType.DMA
    args = [pltpu.with_memory_space_constraint(a, pltpu.HBM) for a in args]
    results = [
        ((depth, cols), F32), ((cols, depth), F32),
        ((rank, cols), F32), ((rank, cols), F32), ((cols, rank), F32), ((cols, rank), F32),
        ((depth, cols), F32), ((cols, depth), F32),
        ((n, depth, cols), BF), ((cols, n * depth), BF),
    ]
    outs = pl.pallas_call(
        functools.partial(update_kernel, nf, nr, n * depth),
        out_shape=[jax.ShapeDtypeStruct(*one) for one in results],
        in_specs=[pl.BlockSpec(memory_space=pltpu.HBM)] * 12,
        out_specs=[pl.BlockSpec(memory_space=pl.ANY)] * 10,
        scratch_shapes=[pltpu.VMEM(*one) for one in results]
        + [
            pltpu.VMEM((tokens, width), BF),
            pltpu.VMEM((2, tokens, cols), BF),
            pltpu.VMEM((2, n, depth, rank), BF),
            pltpu.VMEM((depth, cols), F32), pltpu.VMEM((cols, depth), F32),
            pltpu.VMEM((n, depth, cols), BF), pltpu.VMEM((n, cols, depth) if aligned else (n, depth, cols), BF),
            pltpu.VMEM((tokens, rank), F32), pltpu.VMEM((tokens, rank), BF),
            pltpu.VMEM((nr, nf, rows, span), F32), pltpu.VMEM((nr, nf, rows, span), BF),
            pltpu.VMEM((3, nf, rows, span), BF), pltpu.VMEM((nf, rows, span), BF),
            pltpu.VMEM((nf, rows, span), BF), pltpu.VMEM((2, nr, nf, rows, span), BF),
            pltpu.VMEM((2 * rank, cols), BF), pltpu.VMEM((cols, 2 * rank), BF),
            pltpu.VMEM((rank, 3 * rank), BF), pltpu.VMEM((3 * rank, rank), BF),
            pltpu.VMEM((2, 2, 8, 128), F32),
            dma((10,)), dma((4,)),
            dma, dma((nf,)), dma, dma((3, nf)), dma, dma((nf,)), dma, dma,
            dma((nf,)), dma((2, nf, 3)), dma((nf,)), dma((nf, 2)), dma, dma((nf,)), dma((2,)), dma((nf,)),
            dma, dma((nf,)), dma, dma((nf,)), dma, dma((nf,)), dma, dma((3,)), dma, dma, dma, dma, dma, dma,
        ],
        compiler_params=pltpu.CompilerParams(
            collective_id=0, has_side_effects=True, vmem_limit_bytes=(41 if aligned else 49) * 1024 * 1024
        ),
    )(*[args[k] for k in (0, 3, 1, 2, 4, 5, 6, 7, 8, 9, 10, 11)])
    *rest, query_copy, output_copy = store(outs)
    return (*rest, query_copy.reshape(n * depth, cols), output_copy)


def solution(mesh):
    nf, nr = mesh.shape["fs"], mesh.shape["rep"]
    in_specs = (
        P(("fs", "rep"), None), P(("fs", "rep"), "tp"), P(("fs", "rep"), "tp"), P(("fs", "rep"), None),
        P(("fs", "rep"), "tp"), P("tp", ("fs", "rep")), P(("fs", "rep"), None), P(("fs", "rep"), None),
        P(None, "tp"), P(None, "tp"), P("tp", None), P("tp", None),
    )
    out_specs = (
        P(("fs", "rep"), "tp"), P("tp", ("fs", "rep")), P(None, "tp"), P(None, "tp"), P("tp", None), P("tp", None),
        P(("fs", "rep"), "tp"), P("tp", ("fs", "rep")), P(None, "tp"), P("tp", None),
    )
    return jax.shard_map(
        functools.partial(body, nf, nr), mesh=mesh, in_specs=in_specs, out_specs=out_specs, check_vma=False
    )
```

```python
import functools

import jax
import jax.numpy as jnp
from jax import lax
from jax.experimental import pallas as pl
from jax.experimental.pallas import tpu as pltpu
from jax.sharding import PartitionSpec as P

MESH = pl.DeviceIdType.MESH
BF = jnp.bfloat16
F32 = jnp.float32

REACH = 6.0
SPAN = 120.0
PER_LOG = 1.0 / (2.0 * SPAN * 0.6931471805599453)


def split_parts(wide):
    upper = wide.astype(BF)
    lower = (wide - upper.astype(F32)).astype(BF)
    return (upper, lower)


def encode(weight):
    level = jnp.sqrt(jnp.minimum(jnp.abs(weight), REACH) * (1.0 / REACH))
    size = jnp.exp2(level * (2.0 * SPAN) - SPAN)
    return jnp.where(weight < 0, -size, size).astype(BF)


def decode(code):
    wide = code.astype(F32)
    level = jnp.log(jnp.abs(wide)) * PER_LOG + 0.5
    value = (REACH * level) * level
    return jnp.where(wide < 0, -value, value)


def remote(src, dst, send, recv, where):
    return pltpu.make_async_remote_copy(
        src_ref=src, dst_ref=dst, send_sem=send, recv_sem=recv, device_id=where, device_id_type=MESH
    )


def nth_plane(f, nf, j):
    if j == 0:
        return f, 0
    upper = (2 * f) // nf
    near_end = f + upper * (nf - 1 - 2 * f)
    over = jnp.minimum(1, j // (2 * near_end + 1))
    inner_sign = 1 if j % 2 else -1
    distance = over * (j - near_end) + (1 - over) * ((j + 1) // 2)
    sign = (1 - 2 * upper) * (over + (1 - over) * inner_sign)
    return f + sign * distance, distance


def update_kernel(
    nf, nr, wide,
    x_hbm, bc_hbm, qc_hbm, sh_hbm, wq_hbm, wo_hbm, fq_hbm, fo_hbm, mq_hbm, vq_hbm, mo_hbm, vo_hbm,
    nwq_out, nwo_out, nfq_out, nsq_out, nfo_out, nso_out, stq_out, sto_out, cq_out, co_out,
    nwq_ref, nwo_ref, nfq_ref, nsq_ref, nfo_ref, nso_ref, stq_ref, sto_ref, cq_ref, co_ref,
    xs, cots, fb, wq_ref, wo_ref, cwq, cwo, low, lows, plain_q, plain_o, raws_q, raws_o,
    mine, outgoing, landed, partial, exchanged, whole, dirs, flat, gram_q, gram_o, square,
    loc, put_s, fz_s, fz_r, fn_s, fn_r, fd_s, fd_r, fp_s, fp_r, wn_s, wn_r, wd_s, wd_r, wz_s, wz_r, wb_s, wb_r,
    a_s, a_r, b_s, b_r, c_s, c_r, e_s, e_r, g_s, g_r, h_s, h_r, x_s, x_r,
):
    f, r, t = lax.axis_index("fs"), lax.axis_index("rep"), lax.axis_index("tp")
    near = r + 1 - 2 * lax.rem(r, 2)
    side = lax.rem(r + 2, 4)
    far = 3 - r
    n = nf * nr
    me = f * nr + r
    depth, rank = fq_hbm.shape
    cols = wq_hbm.shape[1]
    tokens = x_hbm.shape[0]
    lane = nr * depth
    rows = rank // nf
    half = nr // 2
    span = cols // half
    peers = (near, side, far)
    aligned = depth % 128 == 0

    local = []

    def fetch(src, dst):
        copy = pltpu.make_async_copy(src, dst, loc.at[len(local)])
        copy.start()
        local.append(copy)
        return copy

    small = [fetch(fq_hbm, fb.at[0, me]), fetch(fo_hbm, fb.at[1, me])]
    weights = [fetch(wq_hbm, wq_ref), fetch(wo_hbm, wo_ref)]
    barrier = pltpu.get_barrier_semaphore()
    for df in range(1, nf):
        pl.semaphore_signal(barrier, inc=1, device_id={"fs": lax.rem(f + df, nf)}, device_id_type=MESH)
    for peer in peers:
        pl.semaphore_signal(barrier, inc=1, device_id={"rep": peer}, device_id_type=MESH)
    pl.semaphore_signal(barrier, inc=1, device_id={"tp": 1 - t}, device_id_type=MESH)
    first, second = t == 0, t == 1
    base = len(local)
    big = []
    for k, (when, src, dst) in enumerate((
        (first, x_hbm, xs), (second, bc_hbm, xs), (first, qc_hbm, cots.at[t]), (second, sh_hbm, cots.at[t]),
    )):
        def make(src=src, dst=dst, k=k):
            return pltpu.make_async_copy(src, dst, loc.at[base + k // 2])

        pl.when(when)(lambda make=make: make().start())
        big.append((when, make))
    local.extend(big[:2])
    moments = [fetch(a, b) for a, b in ((mq_hbm, nfq_ref), (vq_hbm, nsq_ref), (mo_hbm, nfo_ref), (vo_hbm, nso_ref))]
    for copy in small:
        copy.wait()
    pl.semaphore_wait(barrier, nf - 1 + 4)

    def put(src, dst, kind):
        pltpu.make_async_copy(src, dst, put_s.at[kind]).start()

    def gated(when, act):
        if when is None:
            act()
        else:
            pl.when(when)(act)

    def send(src, dst, send_sem, recv_sem, where, when=None):
        gated(when, lambda: remote(src, dst, send_sem, recv_sem, where).start())

    def arrive(ref, sem):
        remote(ref, ref, sem, sem, {"tp": 1 - t}).wait_recv()

    def settle(ref, sem, when=None):
        gated(when, lambda: remote(ref, ref, sem, sem, {"tp": 1 - t}).wait_send())

    def blocks(count):
        return cwq.at[pl.ds(0, count)]

    planes = [nth_plane(f, nf, j) for j in range(nf)]
    for when, src in ((first, sh_hbm), (second, qc_hbm)):
        send(src, cots.at[t], h_s, h_r, {"tp": 1 - t}, when)

    def fpiece(slot, h):
        return fb.at[t, slot, pl.ds(h * (depth // 2), depth // 2)]

    def f_pass(slot):
        send(fb.at[t, slot], fb.at[t, slot], fp_s, fp_r, {"tp": 1 - t})

    def f_relay(p):
        slot = p * nr + r
        for h in range(2):
            for k, peer, piece in ((0, near, h), (1, side, 1 - h)):
                ref = fpiece(slot, piece)
                send(ref, ref, fn_s, fn_r.at[k if piece == k else 2, p], {"rep": peer})

    def f_far(p):
        one, two = p * nr + near, p * nr + side
        for piece, slot, to in ((0, one, side), (1, two, near)):
            ref = fpiece(slot, piece)
            arrive(ref, fn_r.at[piece, p])
            send(ref, ref, fd_s, fd_r.at[p], {"rep": to})
        arrive(fb.at[t, one], fn_r.at[2, p])
        f_pass(one)
        f_pass(two)

    def f_done(p):
        slot = p * nr + far
        arrive(fb.at[t, slot], fd_r.at[p])
        f_pass(slot)

    def wpiece(slot, p):
        ref, count = ((cwq, depth), (cwo, cols if aligned else depth))[p % 2]
        return ref.at[slot, pl.ds(p // 2 * (count // 2), count // 2)]

    def chosen(j, pieces):
        for piece in pieces:
            if piece >= 2 or j == 0:
                yield piece, None
            elif j > 1:
                yield piece, planes[j][1] > 1

    def w_xy(j, pieces):
        p = planes[j][0]
        for piece, when in chosen(j, pieces):
            ref = wpiece(p * nr + r, piece)
            for k, peer in ((0, near), (1, side)):
                at = piece // 2 if piece % 2 == k else 2
                send(ref, ref, wn_s.at[p], wn_r.at[k, p, at], {"rep": peer}, when)

    def w_far(j, pieces):
        p = planes[j][0]
        one, two = p * nr + near, p * nr + side
        for piece, when in chosen(j, pieces):
            k = piece % 2
            ref = wpiece((one, two)[k], piece)
            gated(when, lambda: arrive(ref, wn_r.at[k, p, piece // 2]))
            send(ref, ref, wd_s.at[p], wd_r.at[p, piece // 2], {"rep": (side, near)[k]}, when)

    def w_rest(j):
        p, distance = planes[j]
        for k, ref in ((0, cwo.at[p * nr + near]), (1, cwq.at[p * nr + side])):
            part = wpiece(p * nr + (near, side)[k], 3 - k)
            if j != 1:
                gated(None if j == 0 else distance > 1, lambda: arrive(ref, wn_r.at[k, p, 2]))
            if j > 0:
                gated(distance == 1, lambda: arrive(part, wn_r.at[k, p, 2]))

    def w_last(j, half_of):
        p, distance = planes[j]
        if half_of or j != 1:
            when = None if half_of or j == 0 else distance > 1
            gated(when, lambda: arrive(cwq.at[p * nr + far], wd_r.at[p, half_of]))

    def w_out(j, when=None):
        to = planes[j][0]
        for piece in (2, 3, 0, 1):
            ref = wpiece(me, piece)
            send(ref, ref, wz_s, wz_r.at[f], {"fs": to}, when)

    def w_in(j):
        arrive(blocks(2), wz_r.at[planes[j][0]])

    def w_beside():
        for row in (near, side, far):
            for piece in (0, 1):
                ref = wpiece(f * nr + row, piece)
                send(ref, ref, wb_s.at[0], wb_r.at[f], {"fs": f + 1}, f < nf - 1)
                send(ref, ref, wb_s.at[1], wb_r.at[f], {"fs": f - 1}, f > 0)

    def lowered(j):
        p = planes[j][0]
        block = fb[t, pl.ds(p * nr, nr)].reshape(lane, rank)
        got = jnp.dot(xs[:, pl.ds(pl.multiple_of(p * lane, 128), lane)], block, preferred_element_type=F32)
        if j > 0:
            got = got + low[...]
        if j == nf - 1:
            lows[...] = got.astype(BF)
        else:
            low[...] = got

    for j in range(1, nf):
        to = planes[j][0]
        ref = fb.at[t, me]
        send(ref, ref, fz_s, fz_r.at[f], {"fs": to})
    f_relay(f)
    for copy in weights:
        copy.wait()
    cwq[me] = encode(wq_ref[...])
    cwo[me] = encode(wo_ref[...]) if aligned else encode(wo_ref[...].T)
    w_xy(0, (0,))
    for j in range(1, nf):
        p = planes[j][0]
        slot = p * nr + r
        arrive(fb.at[t, slot], fz_r.at[p])
        f_relay(p)
        f_pass(slot)
        if j == 1:
            w_xy(0, (1,))
        if j == nf - 1:
            for k in range(1, nf):
                w_out(k, planes[k][1] <= 2 if k > 2 else None)
        f_far(planes[j - 1][0])
    for j in range(nf - 2):
        f_done(planes[j][0])
    f_far(planes[nf - 1][0])
    w_xy(0, (2, 3))
    w_far(0, (0, 1))
    for when, make in big:
        pl.when(when)(lambda make=make: make().wait())
    for j in range(nf):
        p = planes[j][0]
        if j >= nf - 2:
            f_done(p)
        lowered(j)
    arrive(cots.at[1 - t], h_r)
    for side_of, quarters in ((side // half, ((2, far), (1, side))), (r // half, ((0, near),))):
        part = lax.dot_general(lows[...], cots[side_of], (((0,), (0,)), ((), ())), preferred_element_type=F32)
        for k in range(half):
            block = part[:, k * span : (k + 1) * span].reshape(nf, rows, span)
            mine[side_of * half + k] = block
            outgoing[side_of * half + k] = block.astype(BF)
        for k, peer in quarters:
            for j in range(nf - 1, -1, -1):
                p = planes[j][0]
                send(outgoing.at[peer, p], landed.at[k, p], a_s, a_r.at[p], {"rep": peer})
    w_last(0, 0)
    w_far(0, (2, 3))
    for j in range(nf - 1, -1, -1):
        p = planes[j][0]
        arrive(landed.at[:, p], a_r.at[p])
        total = mine[r, p] + landed[0, p].astype(F32) + landed[1, p].astype(F32) + landed[2, p].astype(F32)
        if j > 0:
            partial[p] = total.astype(BF)
            send(partial.at[p], exchanged.at[f], b_s, b_r.at[f], {"fs": p})
        else:
            result = total
    def hand(row):
        ref = whole.at[t, row]
        send(ref, ref, g_s, g_r, {"tp": 1 - t}, row // half == 1 - t)

    def weights_o(at, count):
        if aligned:
            return jnp.concatenate([decode(cwo[at + k]) for k in range(count)], axis=1)
        return decode(cwo[pl.ds(at, count)]).reshape(count * depth, cols).T

    def plain(p, at, count):
        plain_q[...] = decode(cwq[pl.ds(at, count)])
        plain_o[...] = weights_o(at, count)

    w_in(1)
    w_xy(1, (2, 3))
    for j in range(1, nf):
        p = planes[j][0]
        arrive(exchanged.at[p], b_r.at[p])
        result = result + exchanged[p].astype(F32)
    whole[t, r, f] = result.astype(BF)
    for j in range(nf):
        p = planes[j][0]
        ref = whole.at[t, r, p]
        if j == 0:
            for i in range(1, nf):
                to = planes[i][0]
                send(ref, ref, c_s, c_r.at[f], {"fs": to})
        else:
            arrive(ref, c_r.at[p])
        for k, peer in ((2, far), (0, near), (1, side)):
            send(ref, ref, e_s, e_r.at[k], {"rep": peer})
        if j == 0:
            for i in range(3, nf):
                w_out(i, planes[i][1] > 2)
            w_far(1, (2, 3))
            w_in(2)
            w_xy(2, (2, 3))
    hand(r)
    w_xy(2, (0, 1))
    w_rest(0)
    w_beside()
    arrive(fb.at[1 - t, pl.ds(0, n - 1)], fp_r)
    for which in range(2):
        block = fb[which].reshape(wide, rank)
        upper, lower = split_parts(lax.dot_general(block, block, (((0,), (0,)), ((), ())), preferred_element_type=F32))
        if which:
            gram_o[...] = jnp.concatenate([upper, lower, upper], axis=0)
        else:
            gram_q[...] = jnp.concatenate([upper, lower, upper], axis=1)
    w_last(0, 1)
    plain(f, f * nr, nr)
    w_far(2, (2, 3))
    for j in range(3, nf):
        w_in(j)
        w_xy(j, (2, 3, 0, 1))
    for k, peer in ((0, near), (1, side), (2, far)):
        arrive(whole.at[t, peer], e_r.at[k])
        hand(peer)
    arrive(whole.at[1 - t, pl.ds(t * half, half)], g_r)
    for copy in moments:
        copy.wait()
    norms = []
    for which, first_ref, second_ref in ((0, nfq_ref, nsq_ref), (1, nfo_ref, nso_ref)):
        proj = jnp.concatenate(
            [whole[which, t * half + k].astype(F32).reshape(rank, span) for k in range(half)], axis=1
        )
        if which:
            proj = proj.T
        moved = 0.9 * first_ref[...] + 0.1 * proj
        spread = 0.95 * second_ref[...] + 0.05 * proj * proj
        first_ref[...] = moved
        second_ref[...] = spread
        way = moved / (jnp.sqrt(spread) + 1e-08)
        upper, lower = split_parts(way)
        if which:
            flat[:, 0:rank] = upper
            flat[:, rank : 2 * rank] = lower
            shaped = jnp.dot(
                jnp.concatenate([upper, upper, lower], axis=1), gram_o[...], preferred_element_type=F32
            )
        else:
            dirs[0:rank] = upper
            dirs[rank : 2 * rank] = lower
            shaped = jnp.dot(
                gram_q[...], jnp.concatenate([upper, upper, lower], axis=0), preferred_element_type=F32
            )
        norms.append(jnp.sum(shaped * way))

    for src, dst in ((nfq_ref, nfq_out), (nsq_ref, nsq_out), (nfo_ref, nfo_out), (nso_ref, nso_out)):
        put(src, dst, 0)
    w_far(2, (0, 1))

    def doubled(which, at, count):
        block = fb[which, pl.ds(at, count)].reshape(count * depth, rank)
        return jnp.concatenate([block, block], axis=1)

    across = (((1,), (1,)), ((), ()))

    def raw_q(at, count):
        return jnp.dot(doubled(0, at, count), dirs[...], preferred_element_type=F32)

    def raw_o(at, count):
        return lax.dot_general(flat[...], doubled(1, at, count), across, preferred_element_type=F32)

    square[0, 0] = jnp.full((8, 128), norms[0], F32)
    square[0, 1] = jnp.full((8, 128), norms[1], F32)
    copy = remote(square.at[0], square.at[1], x_s, x_r, {"tp": 1 - t})
    copy.start()
    for j in range(2):
        p = planes[j][0]
        raws_q[j] = raw_q(p * nr, nr).reshape(nr, depth, cols)
        raws_o[j] = raw_o(p * nr, nr)
    for j in range(3, nf):
        w_far(j, (2, 3))
    copy.wait()
    entries = wide * cols * 2
    scale = [
        1.0 / jnp.sqrt(jnp.maximum(square[0, which, 0:1, 0:1] + square[1, which, 0:1, 0:1], 0.0) / entries + 0.01) for which in range(2)
    ]
    for raw, weight, new_weight, step_ref, which in (
        (raw_q(me, 1), wq_ref, nwq_ref, stq_ref, 0),
        (raw_o(me, 1), wo_ref, nwo_ref, sto_ref, 1),
    ):
        step = raw * scale[which]
        step_ref[...] = step
        new_weight[...] = weight[...] - 0.1 * step

    for src, dst in ((nwq_ref, nwq_out), (nwo_ref, nwo_out), (stq_ref, stq_out), (sto_ref, sto_out)):
        put(src, dst, 1)
    rate = [0.1 * scale[which] for which in range(2)]

    def finish(at, count, j=nf):
        old = plain_q[...] if j == 0 else decode(cwq[pl.ds(at, count)])
        raw = raws_q[j] if j < 2 else raw_q(at, count).reshape(count, depth, cols)
        cq_ref[pl.ds(at, count)] = (old - rate[0] * raw).astype(BF)
        old = plain_o[...] if j == 0 else weights_o(at, count)
        raw = raws_o[j] if j < 2 else raw_o(at, count)
        across_at = pl.ds(pl.multiple_of(at * depth, 128), count * depth)
        co_ref[:, across_at] = (old - rate[1] * raw).astype(BF)
        block = pl.ds(at, count)
        put(cq_ref.at[block], cq_out.at[block], 2)
        block = pl.ds(pl.multiple_of(at * depth, 128), count * depth)
        put(co_ref.at[:, block], co_out.at[:, block], 3)

    for j in range(nf - 1):
        p = planes[j][0]
        if j > 0:
            w_rest(j)
            w_last(j, 0)
            w_last(j, 1)
        if j == 1:
            for step, when in ((1, f < nf - 1), (-1, f > 0)):
                gated(when, lambda: arrive(blocks(3), wb_r.at[f + step]))
        if j == nf - 2:
            for i in range(3, nf):
                w_far(i, (0, 1))
        finish(p * nr, nr, j)
    p = planes[nf - 1][0]
    w_rest(nf - 1)
    if aligned:
        finish(p * nr + r // 2 * 2, 2)
    w_last(nf - 1, 0)
    w_last(nf - 1, 1)
    if aligned:
        finish(p * nr + far // 2 * 2, 2)
    else:
        finish(p * nr, nr)
    for kind, ref in ((0, cq_ref), (1, blocks(8)), (2, cq_ref), (3, co_ref)):
        pltpu.make_async_copy(ref, ref, put_s.at[kind]).wait()
    settle(fb.at[t, pl.ds(0, nf - 1)], fz_s)
    settle(fb.at[t, pl.ds(0, 2 * nf)], fn_s)
    settle(fb.at[t, pl.ds(0, nf)], fd_s)
    settle(fb.at[t, pl.ds(0, n - 1)], fp_s)
    for j in range(nf):
        p, distance = planes[j]
        if j != 1:
            full = None if j == 0 else distance > 1
            settle(blocks(4), wn_s.at[p], full)
            settle(blocks(2), wd_s.at[p], full)
        if j > 0:
            settle(blocks(2), wn_s.at[p], distance == 1)
            settle(blocks(1), wd_s.at[p], distance == 1)
    settle(blocks(2 * (nf - 1)), wz_s)
    settle(blocks(3), wb_s.at[0], f < nf - 1)
    settle(blocks(3), wb_s.at[1], f > 0)
    settle(outgoing.at[pl.ds(0, 3)], a_s)
    settle(partial.at[pl.ds(0, nf - 1)], b_s)
    settle(whole.at[t, r, pl.ds(0, nf - 1)], c_s)
    settle(whole.at[t, pl.ds(0, 3)], e_s)
    settle(whole.at[t, pl.ds(0, half)], g_s)
    settle(cots.at[t], h_s)


def store_kernel(count, *refs):
    ins, outs, sems = refs[:count], refs[count : 2 * count], refs[2 * count]
    copies = [pltpu.make_async_copy(ins[k], outs[k], sems.at[k]) for k in range(count)]
    for copy in copies:
        copy.start()
    for copy in copies:
        copy.wait()


def store(arrays):
    count = len(arrays)
    return pl.pallas_call(
        functools.partial(store_kernel, count),
        out_shape=[jax.ShapeDtypeStruct(a.shape, a.dtype) for a in arrays],
        in_specs=[pl.BlockSpec(memory_space=pl.ANY)] * count,
        out_specs=[pl.BlockSpec(memory_space=pl.ANY)] * count,
        scratch_shapes=[pltpu.SemaphoreType.DMA((count,))],
        compiler_params=pltpu.CompilerParams(vmem_limit_bytes=16 * 1024 * 1024),
    )(*arrays)


def body(nf, nr, *args):
    saved_input, query_cotangent, saved_heads, block_cotangent, query_weight, output_weight = args[:6]
    query_factor, output_factor, query_first, query_second, output_first, output_second = args[6:]
    n = nf * nr
    depth, rank = query_factor.shape
    cols = query_weight.shape[1]
    tokens, width = saved_input.shape
    rows = rank // nf
    span = 2 * cols // nr
    aligned = depth % 128 == 0
    dma = pltpu.SemaphoreType.DMA
    args = [pltpu.with_memory_space_constraint(a, pltpu.HBM) for a in args]
    results = [
        ((depth, cols), F32), ((cols, depth), F32),
        ((rank, cols), F32), ((rank, cols), F32), ((cols, rank), F32), ((cols, rank), F32),
        ((depth, cols), F32), ((cols, depth), F32),
        ((n, depth, cols), BF), ((cols, n * depth), BF),
    ]
    outs = pl.pallas_call(
        functools.partial(update_kernel, nf, nr, n * depth),
        out_shape=[jax.ShapeDtypeStruct(*one) for one in results],
        in_specs=[pl.BlockSpec(memory_space=pltpu.HBM)] * 12,
        out_specs=[pl.BlockSpec(memory_space=pl.ANY)] * 10,
        scratch_shapes=[pltpu.VMEM(*one) for one in results]
        + [
            pltpu.VMEM((tokens, width), BF),
            pltpu.VMEM((2, tokens, cols), BF),
            pltpu.VMEM((2, n, depth, rank), BF),
            pltpu.VMEM((depth, cols), F32), pltpu.VMEM((cols, depth), F32),
            pltpu.VMEM((n, depth, cols), BF), pltpu.VMEM((n, cols, depth) if aligned else (n, depth, cols), BF),
            pltpu.VMEM((tokens, rank), F32), pltpu.VMEM((tokens, rank), BF),
            pltpu.VMEM((nr, depth, cols), F32), pltpu.VMEM((cols, nr * depth), F32),
            pltpu.VMEM((2, nr, depth, cols), F32), pltpu.VMEM((2, cols, nr * depth), F32),
            pltpu.VMEM((nr, nf, rows, span), F32), pltpu.VMEM((nr, nf, rows, span), BF),
            pltpu.VMEM((3, nf, rows, span), BF), pltpu.VMEM((nf, rows, span), BF),
            pltpu.VMEM((nf, rows, span), BF), pltpu.VMEM((2, nr, nf, rows, span), BF),
            pltpu.VMEM((2 * rank, cols), BF), pltpu.VMEM((cols, 2 * rank), BF),
            pltpu.VMEM((rank, 3 * rank), BF), pltpu.VMEM((3 * rank, rank), BF),
            pltpu.VMEM((2, 2, 8, 128), F32),
            dma((10,)), dma((4,)),
            dma, dma((nf,)), dma, dma((3, nf)), dma, dma((nf,)), dma, dma,
            dma((nf,)), dma((2, nf, 3)), dma((nf,)), dma((nf, 2)), dma, dma((nf,)), dma((2,)), dma((nf,)),
            dma, dma((nf,)), dma, dma((nf,)), dma, dma((nf,)), dma, dma((3,)), dma, dma, dma, dma, dma, dma,
        ],
        compiler_params=pltpu.CompilerParams(
            collective_id=0, has_side_effects=True, vmem_limit_bytes=(46 if aligned else 54) * 1024 * 1024
        ),
    )(*[args[k] for k in (0, 3, 1, 2, 4, 5, 6, 7, 8, 9, 10, 11)])
    *rest, query_copy, output_copy = store(outs)
    return (*rest, query_copy.reshape(n * depth, cols), output_copy)


def solution(mesh):
    nf, nr = mesh.shape["fs"], mesh.shape["rep"]
    in_specs = (
        P(("fs", "rep"), None), P(("fs", "rep"), "tp"), P(("fs", "rep"), "tp"), P(("fs", "rep"), None),
        P(("fs", "rep"), "tp"), P("tp", ("fs", "rep")), P(("fs", "rep"), None), P(("fs", "rep"), None),
        P(None, "tp"), P(None, "tp"), P("tp", None), P("tp", None),
    )
    out_specs = (
        P(("fs", "rep"), "tp"), P("tp", ("fs", "rep")), P(None, "tp"), P(None, "tp"), P("tp", None), P("tp", None),
        P(("fs", "rep"), "tp"), P("tp", ("fs", "rep")), P(None, "tp"), P("tp", None),
    )
    return jax.shard_map(
        functools.partial(body, nf, nr), mesh=mesh, in_specs=in_specs, out_specs=out_specs, check_vma=False
    )
```

```python
import functools

import jax
import jax.numpy as jnp
from jax import lax
from jax.experimental import pallas as pl
from jax.experimental.pallas import tpu as pltpu
from jax.sharding import PartitionSpec as P

MESH = pl.DeviceIdType.MESH
BF = jnp.bfloat16
F32 = jnp.float32

REACH = 6.0
SPAN = 120.0
PER_LOG = 1.0 / (2.0 * SPAN * 0.6931471805599453)


def split_parts(wide):
    upper = wide.astype(BF)
    lower = (wide - upper.astype(F32)).astype(BF)
    return (upper, lower)


def encode(weight):
    level = jnp.sqrt(jnp.minimum(jnp.abs(weight), REACH) * (1.0 / REACH))
    size = jnp.exp2(level * (2.0 * SPAN) - SPAN)
    return jnp.where(weight < 0, -size, size).astype(BF)


def decode(code):
    wide = code.astype(F32)
    level = jnp.log(jnp.abs(wide)) * PER_LOG + 0.5
    value = (REACH * level) * level
    return jnp.where(wide < 0, -value, value)


def remote(src, dst, send, recv, where):
    return pltpu.make_async_remote_copy(
        src_ref=src, dst_ref=dst, send_sem=send, recv_sem=recv, device_id=where, device_id_type=MESH
    )


def nth_plane(f, nf, j):
    if j == 0:
        return f, 0
    upper = (2 * f) // nf
    near_end = f + upper * (nf - 1 - 2 * f)
    over = jnp.minimum(1, j // (2 * near_end + 1))
    inner_sign = 1 if j % 2 else -1
    distance = over * (j - near_end) + (1 - over) * ((j + 1) // 2)
    sign = (1 - 2 * upper) * (over + (1 - over) * inner_sign)
    return f + sign * distance, distance


def update_kernel(
    nf, nr, wide,
    x_hbm, bc_hbm, qc_hbm, sh_hbm, wq_hbm, wo_hbm, fq_hbm, fo_hbm, mq_hbm, vq_hbm, mo_hbm, vo_hbm,
    nwq_out, nwo_out, nfq_out, nsq_out, nfo_out, nso_out, stq_out, sto_out, cq_out, co_out,
    nwq_ref, nwo_ref, nfq_ref, nsq_ref, nfo_ref, nso_ref, stq_ref, sto_ref, cq_ref, co_ref,
    xs, cots, fb, wq_ref, wo_ref, cwq, cwo, low, lows, plain_q, plain_o, raws_q, raws_o,
    mine, outgoing, landed, partial, exchanged, whole, dirs, flat, gram_q, gram_o, square,
    loc, put_s, fz_s, fz_r, fn_s, fn_r, fd_s, fd_r, fp_s, fp_r, wn_s, wn_r, wd_s, wd_r, wz_s, wz_r, wb_s, wb_r,
    a_s, a_r, b_s, b_r, c_s, c_r, e_s, e_r, g_s, g_r, h_s, h_r, x_s, x_r,
):
    f, r, t = lax.axis_index("fs"), lax.axis_index("rep"), lax.axis_index("tp")
    near = r + 1 - 2 * lax.rem(r, 2)
    side = lax.rem(r + 2, 4)
    far = 3 - r
    n = nf * nr
    me = f * nr + r
    depth, rank = fq_hbm.shape
    cols = wq_hbm.shape[1]
    tokens = x_hbm.shape[0]
    lane = nr * depth
    rows = rank // nf
    half = nr // 2
    span = cols // half
    peers = (near, side, far)
    aligned = depth % 128 == 0

    local = []

    def fetch(src, dst):
        copy = pltpu.make_async_copy(src, dst, loc.at[len(local)])
        copy.start()
        local.append(copy)
        return copy

    small = [fetch(fq_hbm, fb.at[0, me]), fetch(fo_hbm, fb.at[1, me])]
    weights = [fetch(wq_hbm, wq_ref), fetch(wo_hbm, wo_ref)]
    barrier = pltpu.get_barrier_semaphore()
    for df in range(1, nf):
        pl.semaphore_signal(barrier, inc=1, device_id={"fs": lax.rem(f + df, nf)}, device_id_type=MESH)
    for peer in peers:
        pl.semaphore_signal(barrier, inc=1, device_id={"rep": peer}, device_id_type=MESH)
    pl.semaphore_signal(barrier, inc=1, device_id={"tp": 1 - t}, device_id_type=MESH)
    first, second = t == 0, t == 1
    base = len(local)
    big = []
    for k, (when, src, dst) in enumerate((
        (first, x_hbm, xs), (second, bc_hbm, xs), (first, qc_hbm, cots.at[t]), (second, sh_hbm, cots.at[t]),
    )):
        def make(src=src, dst=dst, k=k):
            return pltpu.make_async_copy(src, dst, loc.at[base + k // 2])

        pl.when(when)(lambda make=make: make().start())
        big.append((when, make))
    local.extend(big[:2])
    moments = [fetch(a, b) for a, b in ((mq_hbm, nfq_ref), (vq_hbm, nsq_ref), (mo_hbm, nfo_ref), (vo_hbm, nso_ref))]
    for copy in small:
        copy.wait()
    pl.semaphore_wait(barrier, nf - 1 + 4)

    def put(src, dst, kind):
        pltpu.make_async_copy(src, dst, put_s.at[kind]).start()

    def gated(when, act):
        if when is None:
            act()
        else:
            pl.when(when)(act)

    def send(src, dst, send_sem, recv_sem, where, when=None):
        gated(when, lambda: remote(src, dst, send_sem, recv_sem, where).start())

    def arrive(ref, sem):
        remote(ref, ref, sem, sem, {"tp": 1 - t}).wait_recv()

    def settle(ref, sem, when=None):
        gated(when, lambda: remote(ref, ref, sem, sem, {"tp": 1 - t}).wait_send())

    def blocks(count):
        return cwq.at[pl.ds(0, count)]

    planes = [nth_plane(f, nf, j) for j in range(nf)]
    for when, src in ((first, sh_hbm), (second, qc_hbm)):
        send(src, cots.at[t], h_s, h_r, {"tp": 1 - t}, when)

    def fpiece(slot, h):
        return fb.at[t, slot, pl.ds(h * (depth // 2), depth // 2)]

    def f_pass(slot):
        send(fb.at[t, slot], fb.at[t, slot], fp_s, fp_r, {"tp": 1 - t})

    def f_relay(p):
        slot = p * nr + r
        for h in range(2):
            for k, peer, piece in ((0, near, h), (1, side, 1 - h)):
                ref = fpiece(slot, piece)
                send(ref, ref, fn_s, fn_r.at[k if piece == k else 2, p], {"rep": peer})

    def f_far(p):
        one, two = p * nr + near, p * nr + side
        for piece, slot, to in ((0, one, side), (1, two, near)):
            ref = fpiece(slot, piece)
            arrive(ref, fn_r.at[piece, p])
            send(ref, ref, fd_s, fd_r.at[p], {"rep": to})
        arrive(fb.at[t, one], fn_r.at[2, p])
        f_pass(one)
        f_pass(two)

    def f_done(p):
        slot = p * nr + far
        arrive(fb.at[t, slot], fd_r.at[p])
        f_pass(slot)

    def wpiece(slot, p):
        ref, count = ((cwq, depth), (cwo, cols if aligned else depth))[p % 2]
        return ref.at[slot, pl.ds(p // 2 * (count // 2), count // 2)]

    def chosen(j, pieces):
        for piece in pieces:
            if piece >= 2 or j == 0:
                yield piece, None
            elif j > 1:
                yield piece, planes[j][1] > 1

    def w_xy(j, pieces):
        p = planes[j][0]
        for piece, when in chosen(j, pieces):
            ref = wpiece(p * nr + r, piece)
            for k, peer in ((0, near), (1, side)):
                at = piece // 2 if piece % 2 == k else 2
                send(ref, ref, wn_s.at[p], wn_r.at[k, p, at], {"rep": peer}, when)

    def w_far(j, pieces):
        p = planes[j][0]
        one, two = p * nr + near, p * nr + side
        for piece, when in chosen(j, pieces):
            k = piece % 2
            ref = wpiece((one, two)[k], piece)
            gated(when, lambda: arrive(ref, wn_r.at[k, p, piece // 2]))
            send(ref, ref, wd_s.at[p], wd_r.at[p, piece // 2], {"rep": (side, near)[k]}, when)

    def w_rest(j):
        p, distance = planes[j]
        for k, ref in ((0, cwo.at[p * nr + near]), (1, cwq.at[p * nr + side])):
            part = wpiece(p * nr + (near, side)[k], 3 - k)
            if j != 1:
                gated(None if j == 0 else distance > 1, lambda: arrive(ref, wn_r.at[k, p, 2]))
            if j > 0:
                gated(distance == 1, lambda: arrive(part, wn_r.at[k, p, 2]))

    def w_last(j, half_of):
        p, distance = planes[j]
        if half_of or j != 1:
            when = None if half_of or j == 0 else distance > 1
            gated(when, lambda: arrive(cwq.at[p * nr + far], wd_r.at[p, half_of]))

    def w_out(j, when=None):
        to = planes[j][0]
        for piece in (2, 3, 0, 1):
            ref = wpiece(me, piece)
            send(ref, ref, wz_s, wz_r.at[f], {"fs": to}, when)

    def w_in(j):
        arrive(blocks(2), wz_r.at[planes[j][0]])

    def w_beside():
        for row in (near, side, far):
            for piece in (0, 1):
                ref = wpiece(f * nr + row, piece)
                send(ref, ref, wb_s.at[0], wb_r.at[f], {"fs": f + 1}, f < nf - 1)
                send(ref, ref, wb_s.at[1], wb_r.at[f], {"fs": f - 1}, f > 0)

    def lowered(j):
        p = planes[j][0]
        block = fb[t, pl.ds(p * nr, nr)].reshape(lane, rank)
        got = jnp.dot(xs[:, pl.ds(pl.multiple_of(p * lane, 128), lane)], block, preferred_element_type=F32)
        if j > 0:
            got = got + low[...]
        if j == nf - 1:
            lows[...] = got.astype(BF)
        else:
            low[...] = got

    for j in range(1, nf):
        to = planes[j][0]
        ref = fb.at[t, me]
        send(ref, ref, fz_s, fz_r.at[f], {"fs": to})
    f_relay(f)
    for copy in weights:
        copy.wait()
    cwq[me] = encode(wq_ref[...])
    cwo[me] = encode(wo_ref[...]) if aligned else encode(wo_ref[...].T)
    w_xy(0, (0,))
    for j in range(1, nf):
        p = planes[j][0]
        slot = p * nr + r
        arrive(fb.at[t, slot], fz_r.at[p])
        f_relay(p)
        f_pass(slot)
        if j == 1:
            w_xy(0, (1,))
        if j == nf - 1:
            for k in range(1, nf):
                w_out(k, planes[k][1] <= 2 if k > 2 else None)
        if j == nf - 1:
            f_done(f)
            for when, make in big:
                pl.when(when)(lambda make=make: make().wait())
            lowered(0)
        f_far(planes[j - 1][0])
    for j in range(1, nf - 2):
        f_done(planes[j][0])
    f_far(planes[nf - 1][0])
    w_xy(0, (2, 3))
    w_far(0, (0, 1))
    for j in range(1, nf):
        p = planes[j][0]
        if j >= nf - 2:
            f_done(p)
        lowered(j)
    arrive(cots.at[1 - t], h_r)
    for side_of, quarters in ((side // half, ((2, far), (1, side))), (r // half, ((0, near),))):
        part = lax.dot_general(lows[...], cots[side_of], (((0,), (0,)), ((), ())), preferred_element_type=F32)
        for k in range(half):
            block = part[:, k * span : (k + 1) * span].reshape(nf, rows, span)
            mine[side_of * half + k] = block
            outgoing[side_of * half + k] = block.astype(BF)
        for k, peer in quarters:
            for j in range(nf - 1, -1, -1):
                p = planes[j][0]
                send(outgoing.at[peer, p], landed.at[k, p], a_s, a_r.at[p], {"rep": peer})
    w_last(0, 0)
    w_far(0, (2, 3))
    for j in range(nf - 1, -1, -1):
        p = planes[j][0]
        arrive(landed.at[:, p], a_r.at[p])
        total = mine[r, p] + landed[0, p].astype(F32) + landed[1, p].astype(F32) + landed[2, p].astype(F32)
        if j > 0:
            partial[p] = total.astype(BF)
            send(partial.at[p], exchanged.at[f], b_s, b_r.at[f], {"fs": p})
        else:
            result = total
    def hand(row):
        ref = whole.at[t, row]
        send(ref, ref, g_s, g_r, {"tp": 1 - t}, row // half == 1 - t)

    def weights_o(at, count):
        if aligned:
            return jnp.concatenate([decode(cwo[at + k]) for k in range(count)], axis=1)
        return decode(cwo[pl.ds(at, count)]).reshape(count * depth, cols).T

    def plain(p, at, count):
        plain_q[...] = decode(cwq[pl.ds(at, count)])
        plain_o[...] = weights_o(at, count)

    w_in(1)
    w_xy(1, (2, 3))
    for j in range(1, nf):
        p = planes[j][0]
        arrive(exchanged.at[p], b_r.at[p])
        result = result + exchanged[p].astype(F32)
    whole[t, r, f] = result.astype(BF)
    for j in range(nf):
        p = planes[j][0]
        ref = whole.at[t, r, p]
        if j == 0:
            for i in range(1, nf):
                to = planes[i][0]
                send(ref, ref, c_s, c_r.at[f], {"fs": to})
        else:
            arrive(ref, c_r.at[p])
        for k, peer in ((2, far), (0, near), (1, side)):
            send(ref, ref, e_s, e_r.at[k], {"rep": peer})
        if j == 0:
            for i in range(3, nf):
                w_out(i, planes[i][1] > 2)
            w_far(1, (2, 3))
            w_in(2)
            w_xy(2, (2, 3))
    hand(r)
    w_xy(2, (0, 1))
    w_rest(0)
    arrive(fb.at[1 - t, pl.ds(0, n - 1)], fp_r)
    for which in range(2):
        block = fb[which].reshape(wide, rank)
        upper, lower = split_parts(lax.dot_general(block, block, (((0,), (0,)), ((), ())), preferred_element_type=F32))
        if which:
            gram_o[...] = jnp.concatenate([upper, lower, upper], axis=0)
        else:
            gram_q[...] = jnp.concatenate([upper, lower, upper], axis=1)
    w_last(0, 1)
    plain(f, f * nr, nr)
    w_beside()
    w_far(2, (2, 3))
    for j in range(3, nf):
        w_in(j)
        w_xy(j, (2, 3, 0, 1))
    for k, peer in ((0, near), (1, side), (2, far)):
        arrive(whole.at[t, peer], e_r.at[k])
        hand(peer)
    arrive(whole.at[1 - t, pl.ds(t * half, half)], g_r)
    for copy in moments:
        copy.wait()
    norms = []
    for which, first_ref, second_ref in ((0, nfq_ref, nsq_ref), (1, nfo_ref, nso_ref)):
        proj = jnp.concatenate(
            [whole[which, t * half + k].astype(F32).reshape(rank, span) for k in range(half)], axis=1
        )
        if which:
            proj = proj.T
        moved = 0.9 * first_ref[...] + 0.1 * proj
        spread = 0.95 * second_ref[...] + 0.05 * proj * proj
        first_ref[...] = moved
        second_ref[...] = spread
        way = moved / (jnp.sqrt(spread) + 1e-08)
        upper, lower = split_parts(way)
        if which:
            flat[:, 0:rank] = upper
            flat[:, rank : 2 * rank] = lower
            shaped = jnp.dot(
                jnp.concatenate([upper, upper, lower], axis=1), gram_o[...], preferred_element_type=F32
            )
        else:
            dirs[0:rank] = upper
            dirs[rank : 2 * rank] = lower
            shaped = jnp.dot(
                gram_q[...], jnp.concatenate([upper, upper, lower], axis=0), preferred_element_type=F32
            )
        norms.append(jnp.sum(shaped * way))

    for src, dst in ((nfq_ref, nfq_out), (nsq_ref, nsq_out), (nfo_ref, nfo_out), (nso_ref, nso_out)):
        put(src, dst, 0)
    w_far(2, (0, 1))

    def doubled(which, at, count):
        block = fb[which, pl.ds(at, count)].reshape(count * depth, rank)
        return jnp.concatenate([block, block], axis=1)

    across = (((1,), (1,)), ((), ()))

    def raw_q(at, count):
        return jnp.dot(doubled(0, at, count), dirs[...], preferred_element_type=F32)

    def raw_o(at, count):
        return lax.dot_general(flat[...], doubled(1, at, count), across, preferred_element_type=F32)

    square[0, 0] = jnp.full((8, 128), norms[0], F32)
    square[0, 1] = jnp.full((8, 128), norms[1], F32)
    copy = remote(square.at[0], square.at[1], x_s, x_r, {"tp": 1 - t})
    copy.start()
    for j in range(3, nf):
        w_far(j, (2, 3))
    for j in range(2):
        p = planes[j][0]
        raws_q[j] = raw_q(p * nr, nr).reshape(nr, depth, cols)
        raws_o[j] = raw_o(p * nr, nr)
    for j in range(3, nf):
        w_far(j, (0, 1))
    copy.wait()
    entries = wide * cols * 2
    scale = [
        1.0 / jnp.sqrt(jnp.maximum(square[0, which, 0:1, 0:1] + square[1, which, 0:1, 0:1], 0.0) / entries + 0.01) for which in range(2)
    ]
    for raw, weight, new_weight, step_ref, which in (
        (raw_q(me, 1), wq_ref, nwq_ref, stq_ref, 0),
        (raw_o(me, 1), wo_ref, nwo_ref, sto_ref, 1),
    ):
        step = raw * scale[which]
        step_ref[...] = step
        new_weight[...] = weight[...] - 0.1 * step

    for src, dst in ((nwq_ref, nwq_out), (nwo_ref, nwo_out), (stq_ref, stq_out), (sto_ref, sto_out)):
        put(src, dst, 1)
    rate = [0.1 * scale[which] for which in range(2)]

    def finish(at, count, j=nf):
        old = plain_q[...] if j == 0 else decode(cwq[pl.ds(at, count)])
        raw = raws_q[j] if j < 2 else raw_q(at, count).reshape(count, depth, cols)
        cq_ref[pl.ds(at, count)] = (old - rate[0] * raw).astype(BF)
        old = plain_o[...] if j == 0 else weights_o(at, count)
        raw = raws_o[j] if j < 2 else raw_o(at, count)
        across_at = pl.ds(pl.multiple_of(at * depth, 128), count * depth)
        co_ref[:, across_at] = (old - rate[1] * raw).astype(BF)
        block = pl.ds(at, count)
        put(cq_ref.at[block], cq_out.at[block], 2)
        block = pl.ds(pl.multiple_of(at * depth, 128), count * depth)
        put(co_ref.at[:, block], co_out.at[:, block], 3)

    for j in range(nf - 1):
        p = planes[j][0]
        if j > 0:
            w_rest(j)
            w_last(j, 0)
            w_last(j, 1)
        if j == 1:
            for step, when in ((1, f < nf - 1), (-1, f > 0)):
                gated(when, lambda: arrive(blocks(3), wb_r.at[f + step]))
        finish(p * nr, nr, j)
    p = planes[nf - 1][0]
    w_rest(nf - 1)
    if aligned:
        finish(p * nr + r // 2 * 2, 2)
    w_last(nf - 1, 0)
    w_last(nf - 1, 1)
    if aligned:
        finish(p * nr + far // 2 * 2, 2)
    else:
        finish(p * nr, nr)
    for kind, ref in ((0, cq_ref), (1, blocks(8)), (2, cq_ref), (3, co_ref)):
        pltpu.make_async_copy(ref, ref, put_s.at[kind]).wait()
    settle(fb.at[t, pl.ds(0, nf - 1)], fz_s)
    settle(fb.at[t, pl.ds(0, 2 * nf)], fn_s)
    settle(fb.at[t, pl.ds(0, nf)], fd_s)
    settle(fb.at[t, pl.ds(0, n - 1)], fp_s)
    for j in range(nf):
        p, distance = planes[j]
        if j != 1:
            full = None if j == 0 else distance > 1
            settle(blocks(4), wn_s.at[p], full)
            settle(blocks(2), wd_s.at[p], full)
        if j > 0:
            settle(blocks(2), wn_s.at[p], distance == 1)
            settle(blocks(1), wd_s.at[p], distance == 1)
    settle(blocks(2 * (nf - 1)), wz_s)
    settle(blocks(3), wb_s.at[0], f < nf - 1)
    settle(blocks(3), wb_s.at[1], f > 0)
    settle(outgoing.at[pl.ds(0, 3)], a_s)
    settle(partial.at[pl.ds(0, nf - 1)], b_s)
    settle(whole.at[t, r, pl.ds(0, nf - 1)], c_s)
    settle(whole.at[t, pl.ds(0, 3)], e_s)
    settle(whole.at[t, pl.ds(0, half)], g_s)
    settle(cots.at[t], h_s)


def store_kernel(count, *refs):
    ins, outs, sems = refs[:count], refs[count : 2 * count], refs[2 * count]
    copies = [pltpu.make_async_copy(ins[k], outs[k], sems.at[k]) for k in range(count)]
    for copy in copies:
        copy.start()
    for copy in copies:
        copy.wait()


def store(arrays):
    count = len(arrays)
    return pl.pallas_call(
        functools.partial(store_kernel, count),
        out_shape=[jax.ShapeDtypeStruct(a.shape, a.dtype) for a in arrays],
        in_specs=[pl.BlockSpec(memory_space=pl.ANY)] * count,
        out_specs=[pl.BlockSpec(memory_space=pl.ANY)] * count,
        scratch_shapes=[pltpu.SemaphoreType.DMA((count,))],
        compiler_params=pltpu.CompilerParams(vmem_limit_bytes=16 * 1024 * 1024),
    )(*arrays)


def body(nf, nr, *args):
    saved_input, query_cotangent, saved_heads, block_cotangent, query_weight, output_weight = args[:6]
    query_factor, output_factor, query_first, query_second, output_first, output_second = args[6:]
    n = nf * nr
    depth, rank = query_factor.shape
    cols = query_weight.shape[1]
    tokens, width = saved_input.shape
    rows = rank // nf
    span = 2 * cols // nr
    aligned = depth % 128 == 0
    dma = pltpu.SemaphoreType.DMA
    args = [pltpu.with_memory_space_constraint(a, pltpu.HBM) for a in args]
    results = [
        ((depth, cols), F32), ((cols, depth), F32),
        ((rank, cols), F32), ((rank, cols), F32), ((cols, rank), F32), ((cols, rank), F32),
        ((depth, cols), F32), ((cols, depth), F32),
        ((n, depth, cols), BF), ((cols, n * depth), BF),
    ]
    outs = pl.pallas_call(
        functools.partial(update_kernel, nf, nr, n * depth),
        out_shape=[jax.ShapeDtypeStruct(*one) for one in results],
        in_specs=[pl.BlockSpec(memory_space=pltpu.HBM)] * 12,
        out_specs=[pl.BlockSpec(memory_space=pl.ANY)] * 10,
        scratch_shapes=[pltpu.VMEM(*one) for one in results]
        + [
            pltpu.VMEM((tokens, width), BF),
            pltpu.VMEM((2, tokens, cols), BF),
            pltpu.VMEM((2, n, depth, rank), BF),
            pltpu.VMEM((depth, cols), F32), pltpu.VMEM((cols, depth), F32),
            pltpu.VMEM((n, depth, cols), BF), pltpu.VMEM((n, cols, depth) if aligned else (n, depth, cols), BF),
            pltpu.VMEM((tokens, rank), F32), pltpu.VMEM((tokens, rank), BF),
            pltpu.VMEM((nr, depth, cols), F32), pltpu.VMEM((cols, nr * depth), F32),
            pltpu.VMEM((2, nr, depth, cols), F32), pltpu.VMEM((2, cols, nr * depth), F32),
            pltpu.VMEM((nr, nf, rows, span), F32), pltpu.VMEM((nr, nf, rows, span), BF),
            pltpu.VMEM((3, nf, rows, span), BF), pltpu.VMEM((nf, rows, span), BF),
            pltpu.VMEM((nf, rows, span), BF), pltpu.VMEM((2, nr, nf, rows, span), BF),
            pltpu.VMEM((2 * rank, cols), BF), pltpu.VMEM((cols, 2 * rank), BF),
            pltpu.VMEM((rank, 3 * rank), BF), pltpu.VMEM((3 * rank, rank), BF),
            pltpu.VMEM((2, 2, 8, 128), F32),
            dma((10,)), dma((4,)),
            dma, dma((nf,)), dma, dma((3, nf)), dma, dma((nf,)), dma, dma,
            dma((nf,)), dma((2, nf, 3)), dma((nf,)), dma((nf, 2)), dma, dma((nf,)), dma((2,)), dma((nf,)),
            dma, dma((nf,)), dma, dma((nf,)), dma, dma((nf,)), dma, dma((3,)), dma, dma, dma, dma, dma, dma,
        ],
        compiler_params=pltpu.CompilerParams(
            collective_id=0, has_side_effects=True, vmem_limit_bytes=(46 if aligned else 54) * 1024 * 1024
        ),
    )(*[args[k] for k in (0, 3, 1, 2, 4, 5, 6, 7, 8, 9, 10, 11)])
    *rest, query_copy, output_copy = store(outs)
    return (*rest, query_copy.reshape(n * depth, cols), output_copy)


def solution(mesh):
    nf, nr = mesh.shape["fs"], mesh.shape["rep"]
    in_specs = (
        P(("fs", "rep"), None), P(("fs", "rep"), "tp"), P(("fs", "rep"), "tp"), P(("fs", "rep"), None),
        P(("fs", "rep"), "tp"), P("tp", ("fs", "rep")), P(("fs", "rep"), None), P(("fs", "rep"), None),
        P(None, "tp"), P(None, "tp"), P("tp", None), P("tp", None),
    )
    out_specs = (
        P(("fs", "rep"), "tp"), P("tp", ("fs", "rep")), P(None, "tp"), P(None, "tp"), P("tp", None), P("tp", None),
        P(("fs", "rep"), "tp"), P("tp", ("fs", "rep")), P(None, "tp"), P("tp", None),
    )
    return jax.shard_map(
        functools.partial(body, nf, nr), mesh=mesh, in_specs=in_specs, out_specs=out_specs, check_vma=False
    )
```
